256 devices in a mesh: ep: 64 (over z, x, core), tp: 4 (over y).
Axes of the slice: x: 4, y: 4, z: 8, core: 2. Of those that a mesh axis runs over, the one named last changes fastest.
Arguments:
- residual_in: bfloat16 [1024, 2048], P('ep'), may hold values from -6 to 6
- lengths: int32 [1024], P('ep'), may hold values from 1 to 511, as said below
- kv_cache: bfloat16 [1024, 4, 512, 256], P('ep', 'tp'), may hold values from -640 to 640
- norm_gain_attn: float32 [2048], replicated, may hold values from 0.1 to 1.9
- query_weight: bfloat16 [2048, 2048], P(None, 'tp'), may hold values from -0.125 to 0.125
- key_weight: bfloat16 [2048, 512], P(None, 'tp'), may hold values from -0.125 to 0.125
- value_weight: bfloat16 [2048, 512], P(None, 'tp'), may hold values from -0.125 to 0.125
- diff_lambda: float32 [16], P('tp'), may hold values from 0.3 to 0.8
- head_gain: float32 [128], replicated, may hold values from 0.1 to 1.9
- out_weight: bfloat16 [2048, 2048], P(None, 'tp'), may hold values from -0.125 to 0.125
- norm_gain_ffn: float32 [2048], replicated, may hold values from 0.1 to 1.9
- route_ids: int32 [1024, 2], P('ep'), may hold values from 0 to 63, as said below
- route_weights: float32 [1024, 2], P('ep'), may hold values from 0.1 to 1
- expert_gate: bfloat16 [64, 2048, 512], P('ep', None, 'tp'), may hold values from -0.125 to 0.125
- expert_up: bfloat16 [64, 2048, 512], P('ep', None, 'tp'), may hold values from -0.125 to 0.125
- expert_down: bfloat16 [64, 512, 2048], P('ep', 'tp'), may hold values from -0.25 to 0.25
- dense_gate: bfloat16 [2048, 8192], P(None, 'ep'), may hold values from -0.125 to 0.125
- dense_up: bfloat16 [2048, 8192], P(None, 'ep'), may hold values from -0.125 to 0.125
- dense_down: bfloat16 [8192, 2048], P('ep'), may hold values from -0.0625 to 0.0625
- dense_mix: float32 [2048], replicated, may hold values from -0.125 to 0.125
Outputs:
- layer_out: bfloat16 [1024, 2048], P('ep', 'tp')
- new_rows: bfloat16 [1024, 4, 256], P('ep', 'tp')
The draws below stay inside these ranges and needn't reach their ends.
Inputs may be any that keep to these rules, and one draw needn't show every extreme that they name: The new token stands at position lengths[b]; some sequence holds 511 positions in every draw. `route_ids`: each row names 2 different experts from one group; the groups are the 4 runs of consecutive expert numbers of equal size. Among the rows of one index of ep no expert is named more than 2 times, and some expert exactly 2 times.
All inputs are finite; a program needn't handle non-finite values.
Results may differ from the reference program's by a relative error of at most 0.008.
The reference program's roundings to bfloat16 on the way count: a program that leaves them out, or rounds other values in their place, can miss the bound.
Values may be sent and summed in bfloat16 or wider, within the bound.
A program may use at most 64 MiB of HBM per device.

```python
import math
import jax
import jax.numpy as jnp
from jax import lax

D = 2048
HEADS = 16
KV_HEADS = 4
QK_DIM = 64
HEAD_DIM = 128
KV_WIDTH = 256
SEQ_DEV = 16
CACHE = 512
TOKENS = 1024
EXPERTS = 64
GROUPS = 4
TOPK = 2
EXP_FF = 512
DENSE_FF = 8192
CAP = 2
N_EP = 64
N_TP = 4


def draw_lengths(key, part):
    raw = jax.random.randint(jax.random.fold_in(key, 21), (TOKENS,), 0, CACHE - 1)
    factor = jax.random.randint(jax.random.fold_in(key, 22), (TOKENS // SEQ_DEV, 1), 1, 9)
    spread = jnp.broadcast_to(factor, (TOKENS // SEQ_DEV, SEQ_DEV)).reshape(TOKENS)
    counts = 1 + raw * spread // 8
    longest = jax.random.randint(jax.random.fold_in(key, 23), (), 0, TOKENS)
    return jnp.where(jnp.arange(TOKENS, dtype=jnp.int32) == longest, CACHE - 1, counts).astype(jnp.int32)


def draw_kv_cache(key, part):
    base = jnp.clip(jax.random.normal(key, (TOKENS, KV_HEADS, CACHE, KV_WIDTH), jnp.float32), -6.0, 6.0)
    lane = lax.broadcasted_iota(jnp.int32, (1, 1, 1, KV_WIDTH), 3)
    level = jnp.ones((TOKENS, KV_HEADS, 1, 1), jnp.float32)
    factor = jnp.where(lane < 2 * QK_DIM, 1.75 * level, 1.0)
    return (base * factor).astype(jnp.bfloat16)


def draw_route_ids(key, part):
    blocks = TOKENS // SEQ_DEV
    per_group = EXPERTS // GROUPS
    busy_rows = CAP * per_group // TOPK
    busy = jax.random.randint(jax.random.fold_in(key, 41), (blocks, 1), 0, GROUPS)
    other = (busy + jax.random.randint(jax.random.fold_in(key, 42), (blocks, SEQ_DEV), 1, GROUPS)) % GROUPS
    place = lax.broadcasted_iota(jnp.int32, (blocks, SEQ_DEV), 1)
    ordered = jnp.where(place < busy_rows, busy, other)
    scores = jax.random.randint(jax.random.fold_in(key, 43), (blocks, SEQ_DEV), 0, 1 << 20) * SEQ_DEV + place
    order = jnp.argsort(scores, axis=1)
    group = jnp.take_along_axis(ordered, order, axis=1)
    member = (group[:, :, None] == jnp.arange(GROUPS, dtype=jnp.int32)[None, None, :]).astype(jnp.int32)
    rank = jnp.sum((jnp.cumsum(member, axis=1) - member) * member, axis=2)
    shift = TOPK * jax.random.randint(jax.random.fold_in(key, 44), (blocks, GROUPS), 0, per_group // TOPK)
    offset = jnp.take_along_axis(shift, group, axis=1)
    first = TOPK * rank + offset
    picks = [group * per_group + (first + step) % per_group for step in range(TOPK)]
    return jnp.stack(picks, axis=-1).reshape(TOKENS, TOPK).astype(jnp.int32)


def level_of(key, shape, shards, low, largest):
    def one(position, shards_of):
        steps = jax.random.uniform(jax.random.fold_in(jax.random.fold_in(key, 6), position), (shards_of,), jnp.float32, low / len(shards), largest / len(shards))
        return jnp.repeat(jnp.exp(steps), shape[position] // shards_of).reshape((-1,) + (1,) * (len(shape) - position - 1))

    level = one(*shards[0])
    for cut in shards[1:]:
        level = level * one(*cut)
    return level


def scatter_about(own_key, dims, scale, most, split=(), kind=jnp.bfloat16):
    level = level_of(own_key, dims, split, -0.22, 0.18) if split else 1.0
    array = jax.random.normal(own_key, dims, jnp.float32) * scale * level
    return jnp.minimum(jnp.maximum(array, -most), most).astype(kind)


def setup_inputs(seed: int = 0) -> dict:
    seeds = jax.random.split(jax.random.key(seed), 21)
    return {
        "residual_in": scatter_about(seeds[0], (TOKENS, D), 1.0, 6.0, ((0, 64),)),
        "lengths": draw_lengths(jax.random.fold_in(seeds[20], 71), 0),
        "kv_cache": draw_kv_cache(jax.random.fold_in(seeds[20], 71), 0),
        "norm_gain_attn": jnp.clip(1.0 + 0.18 * jax.random.normal(seeds[3], (D,), jnp.float32), 0.1, 1.9),
        "query_weight": scatter_about(seeds[4], (D, HEADS * 2 * QK_DIM), D ** -0.5, 0.125, ((1, 4),)),
        "key_weight": scatter_about(seeds[5], (D, KV_HEADS * 2 * QK_DIM), D ** -0.5, 0.125, ((1, 4),)),
        "value_weight": scatter_about(seeds[6], (D, KV_HEADS * HEAD_DIM), D ** -0.5, 0.125, ((1, 4),)),
        "diff_lambda": jnp.clip(0.3 + 0.5 * jax.random.uniform(seeds[7], (HEADS,), jnp.float32) ** level_of(seeds[7], (HEADS,), ((0, 4),), -0.2, 0.2), 0.3, 0.8),
        "head_gain": jnp.clip(1.0 + 0.18 * jax.random.normal(seeds[8], (HEAD_DIM,), jnp.float32), 0.1, 1.9),
        "out_weight": scatter_about(seeds[9], (HEADS * HEAD_DIM, D), (HEADS * HEAD_DIM) ** -0.5, 0.125, ((1, 4),)),
        "norm_gain_ffn": jnp.clip(1.0 + 0.18 * jax.random.normal(seeds[10], (D,), jnp.float32), 0.1, 1.9),
        "route_ids": draw_route_ids(jax.random.fold_in(seeds[20], 71), 0),
        "route_weights": jnp.clip(jnp.exp(math.log(1.0) - 2.3025851 * jax.random.uniform(seeds[12], (TOKENS, TOPK), jnp.float32) ** level_of(seeds[12], (TOKENS, TOPK), ((0, 64),), -0.2, 0.2)), 0.1, 1.0),
        "expert_gate": scatter_about(seeds[13], (EXPERTS, D, EXP_FF), D ** -0.5, 0.125, ((0, 64), (2, 4))),
        "expert_up": scatter_about(seeds[14], (EXPERTS, D, EXP_FF), D ** -0.5, 0.125, ((0, 64), (2, 4))),
        "expert_down": scatter_about(seeds[15], (EXPERTS, EXP_FF, D), EXP_FF ** -0.5, 0.25, ((0, 64), (1, 4))),
        "dense_gate": scatter_about(seeds[16], (D, DENSE_FF), D ** -0.5, 0.125, ((1, 64),)),
        "dense_up": scatter_about(seeds[17], (D, DENSE_FF), D ** -0.5, 0.125, ((1, 64),)),
        "dense_down": scatter_about(seeds[18], (DENSE_FF, D), DENSE_FF ** -0.5, 0.0625, ((0, 64),)),
        "dense_mix": scatter_about(seeds[19], (D,), D ** -0.5, 0.125, (), jnp.float32),
    }


EPS = 1e-06

def rms_rows(values, gain):
    mean_sq = lax.optimization_barrier(jnp.mean(values * values, axis=-1, keepdims=True))
    return values * lax.rsqrt(mean_sq + EPS) * gain

def rotate(vectors, positions):
    half = vectors.shape[-1] // 2
    inverse = 10000.0 ** (-jnp.arange(half, dtype=jnp.float32) / half)
    angle = positions[:, None, None, None] * inverse
    cosine = jnp.cos(angle)
    sine = jnp.sin(angle)
    first = vectors[..., :half]
    second = vectors[..., half:]
    return jnp.concatenate([first * cosine - second * sine, first * sine + second * cosine], axis=-1)

def normalize(scores, latest, valid):
    masked = jnp.where(valid, scores, -jnp.inf)
    top = jnp.maximum(lax.optimization_barrier(jnp.max(masked, axis=-1)), latest)
    raised = jnp.where(valid, jnp.exp(jnp.where(valid, scores, 0.0) - top[..., None]), 0.0)
    raised_new = jnp.exp(latest - top)
    total = lax.optimization_barrier(jnp.sum(raised, axis=-1)) + raised_new
    return (raised / total[..., None], raised_new / total)

def attend(query, fresh, cache, lengths, lam):
    count = fresh.shape[0]
    groups = fresh.shape[1]
    share = query.shape[1] // groups
    scale = QK_DIM ** (-0.5)
    grouped = query.astype(jnp.float32).reshape(count, groups, share, 2, QK_DIM)
    latest = fresh.astype(jnp.float32)
    stored = cache.astype(jnp.float32)
    first = jnp.einsum('bgjd,bgkd->bgjk', grouped[:, :, :, 0], stored[..., :QK_DIM]) * scale
    second = jnp.einsum('bgjd,bgkd->bgjk', grouped[:, :, :, 1], stored[..., QK_DIM:2 * QK_DIM]) * scale
    first_new = jnp.einsum('bgjd,bgd->bgj', grouped[:, :, :, 0], latest[..., :QK_DIM]) * scale
    second_new = jnp.einsum('bgjd,bgd->bgj', grouped[:, :, :, 1], latest[..., QK_DIM:2 * QK_DIM]) * scale
    valid = jnp.arange(cache.shape[2], dtype=jnp.int32)[None, None, None, :] < lengths[:, None, None, None]
    prob_one, prob_one_new = normalize(first, first_new, valid)
    prob_two, prob_two_new = normalize(second, second_new, valid)
    weight = lam.reshape(groups, share)[None, :, :, None]
    mapped = (prob_one - weight * prob_two).astype(jnp.bfloat16)
    mapped_new = (prob_one_new - weight[..., 0] * prob_two_new).astype(jnp.bfloat16)
    output = jnp.einsum('bgjk,bgkd->bgjd', mapped.astype(jnp.float32), stored[..., 2 * QK_DIM:])
    output = output + mapped_new.astype(jnp.float32)[..., None] * latest[:, :, None, 2 * QK_DIM:]
    return output.reshape(count, groups * share, HEAD_DIM)

def reference(residual_in, lengths, kv_cache, norm_gain_attn, query_weight, key_weight, value_weight, diff_lambda, head_gain, out_weight, norm_gain_ffn, route_ids, route_weights, expert_gate, expert_up, expert_down, dense_gate, dense_up, dense_down, dense_mix):
    blocks = TOKENS // SEQ_DEV
    resid = residual_in.astype(jnp.float32)
    normed = rms_rows(resid, norm_gain_attn).astype(jnp.bfloat16)
    positions = lengths.astype(jnp.float32)
    query = jnp.dot(normed, query_weight, preferred_element_type=jnp.float32).reshape(TOKENS, HEADS, 2, QK_DIM)
    query = rotate(query, positions).astype(jnp.bfloat16)
    keys = jnp.dot(normed, key_weight, preferred_element_type=jnp.float32).reshape(TOKENS, KV_HEADS, 2, QK_DIM)
    keys = rotate(keys, positions).astype(jnp.bfloat16).reshape(TOKENS, KV_HEADS, 2 * QK_DIM)
    values = jnp.dot(normed, value_weight, preferred_element_type=jnp.float32).reshape(TOKENS, KV_HEADS, HEAD_DIM).astype(jnp.bfloat16)
    fresh = jnp.concatenate([keys, values], axis=-1)

    def per_block(items):
        return attend(items[0], items[1], items[2], items[3], diff_lambda)
    mixed = lax.map(per_block, (query.reshape(blocks, SEQ_DEV, HEADS, 2, QK_DIM), fresh.reshape(blocks, SEQ_DEV, KV_HEADS, KV_WIDTH), kv_cache.reshape(blocks, SEQ_DEV, KV_HEADS, CACHE, KV_WIDTH), lengths.reshape(blocks, SEQ_DEV)))
    mixed = mixed.reshape(TOKENS, HEADS, HEAD_DIM)
    heads_out = rms_rows(mixed, head_gain).astype(jnp.bfloat16).reshape(TOKENS, HEADS * HEAD_DIM)
    stream = (resid + jnp.dot(heads_out, out_weight, preferred_element_type=jnp.float32)).astype(jnp.bfloat16)
    ffn_in = rms_rows(stream.astype(jnp.float32), norm_gain_ffn).astype(jnp.bfloat16)
    flat_ids = route_ids.reshape(blocks, SEQ_DEV * TOPK)
    member = (flat_ids[..., None] == jnp.arange(EXPERTS, dtype=jnp.int32)[None, None, :]).astype(jnp.int32)
    slot = lax.optimization_barrier(jnp.sum((jnp.cumsum(member, axis=1) - member) * member, axis=2))
    block_of = lax.broadcasted_iota(jnp.int32, (blocks, SEQ_DEV * TOPK), 0)
    place = (flat_ids * N_EP + block_of) * CAP + slot
    owner = block_of * SEQ_DEV + lax.broadcasted_iota(jnp.int32, (blocks, SEQ_DEV * TOPK), 1) // TOPK
    table = jnp.zeros((EXPERTS * N_EP * CAP,), jnp.int32).at[place.reshape(-1)].set(owner.reshape(-1))
    quarter = EXP_FF // N_TP

    def expert_rows(items):
        index, w_gate, w_up, w_down = items
        chosen = ffn_in[index]
        gate = jnp.dot(chosen, w_gate, preferred_element_type=jnp.float32)
        upward = jnp.dot(chosen, w_up, preferred_element_type=jnp.float32)
        hidden = (jax.nn.silu(gate) * upward).astype(jnp.bfloat16)
        total = jnp.zeros((chosen.shape[0], D), jnp.float32)
        for part in range(N_TP):
            piece = jnp.dot(hidden[:, part * quarter:(part + 1) * quarter], w_down[part * quarter:(part + 1) * quarter], preferred_element_type=jnp.float32).astype(jnp.bfloat16)
            total = total + lax.optimization_barrier(piece).astype(jnp.float32)
        return total.astype(jnp.bfloat16)
    results = lax.map(expert_rows, (table.reshape(EXPERTS, N_EP * CAP), expert_gate, expert_up, expert_down))
    flat_results = results.reshape(EXPERTS * N_EP * CAP, D)
    picked = flat_results[place.reshape(TOKENS, TOPK)]
    moe = lax.optimization_barrier(jnp.sum(route_weights[..., None] * picked.astype(jnp.float32), axis=1))
    dense_g = jnp.dot(ffn_in, dense_gate, preferred_element_type=jnp.float32)
    dense_u = jnp.dot(ffn_in, dense_up, preferred_element_type=jnp.float32)
    dense_hidden = (jax.nn.silu(dense_g) * dense_u).astype(jnp.bfloat16)
    dense = jnp.dot(dense_hidden, dense_down, preferred_element_type=jnp.float32)
    mix = jax.nn.sigmoid(lax.optimization_barrier(jnp.sum(ffn_in.astype(jnp.float32) * dense_mix, axis=-1)))
    layer_out = (stream.astype(jnp.float32) + moe + mix[:, None] * dense).astype(jnp.bfloat16)
    return (layer_out, fresh)
```

```python
import jax
import jax.numpy as jnp
from jax import lax
from jax.experimental import pallas as pl
from jax.experimental.pallas import tpu as pltpu
from jax.sharding import PartitionSpec as P

QK_DIM = 64
HEAD_DIM = 128
EPS = 1e-06
MESH = pl.DeviceIdType.MESH
F32 = jnp.float32
BF16 = jnp.bfloat16
NX, NZ, NY, NC = 4, 8, 4, 2
SEQ = 16
D = 2048
Q = 512
INFO = 128
WIDE = D + INFO
FF = 128
X_ORDER = (0, 1, 3, 2)
N_SENDS = 63


def rms_rows(values, gain):
    mean_sq = jnp.mean(values * values, axis=-1, keepdims=True)
    return values * lax.rsqrt(mean_sq + EPS) * gain


def rotate(vectors, positions):
    half = vectors.shape[-1] // 2
    inverse = 10000.0 ** (-jnp.arange(half, dtype=jnp.float32) / half)
    angle = positions[:, None, None, None] * inverse
    cosine = jnp.cos(angle)
    sine = jnp.sin(angle)
    first = vectors[..., :half]
    second = vectors[..., half:]
    return jnp.concatenate(
        [first * cosine - second * sine, first * sine + second * cosine], axis=-1
    )


def normalize(scores, latest, valid):
    masked = jnp.where(valid, scores, -jnp.inf)
    top = jnp.maximum(jnp.max(masked, axis=-1), latest)
    raised = jnp.where(valid, jnp.exp(jnp.where(valid, scores, 0.0) - top[..., None]), 0.0)
    raised_new = jnp.exp(latest - top)
    total = jnp.sum(raised, axis=-1) + raised_new
    return (raised / total[..., None], raised_new / total)


def attend(query, fresh, cache, lengths, lam):
    count = fresh.shape[0]
    groups = fresh.shape[1]
    share = query.shape[1] // groups
    scale = QK_DIM ** (-0.5)
    grouped = query.reshape(count, groups, share, 2, QK_DIM)

    def scores(eq, n, lo):
        keys = (cache if n else fresh)[..., lo * QK_DIM : (lo + 1) * QK_DIM]
        return jnp.einsum(eq, grouped[:, :, :, lo], keys, preferred_element_type=F32) * scale

    first = scores("bgjd,bgkd->bgjk", 1, 0)
    second = scores("bgjd,bgkd->bgjk", 1, 1)
    first_new = scores("bgjd,bgd->bgj", 0, 0)
    second_new = scores("bgjd,bgd->bgj", 0, 1)
    valid = (
        jnp.arange(cache.shape[2], dtype=jnp.int32)[None, None, None, :]
        < lengths[:, None, None, None]
    )
    prob_one, prob_one_new = normalize(first, first_new, valid)
    prob_two, prob_two_new = normalize(second, second_new, valid)
    weight = lam.reshape(groups, share)[None, :, :, None]
    mapped = (prob_one - weight * prob_two).astype(BF16)
    mapped_new = (prob_one_new - weight[..., 0] * prob_two_new).astype(BF16)
    output = jnp.einsum(
        "bgjk,bgkd->bgjd", mapped, cache[..., 2 * QK_DIM :], preferred_element_type=F32
    )
    output = output + mapped_new.astype(F32)[..., None] * fresh[:, :, None, 2 * QK_DIM :].astype(F32)
    return output.reshape(count, groups * share, HEAD_DIM)


def dot(a, b):
    return jnp.dot(a, b, preferred_element_type=F32)


def up(v, n, size):
    return lax.rem(v + (n % size), size)


def tail_kernel(
    heads, resid, gain, mix_w, ids_t, rw_t, wo_h, eg_h, eu_h, ed_h, dg_h, du_h, dd_h, out,
    wo, we, wd, ed, dd, edx, hg, sg, xg, he, hd, st, wc, mc, hx, slots, eo,
    s0, r0, own, s1, r1, bsum, s2, r2,
    lsem, ed_s, ed_r, h_s, h_r, c_s, c_r, g_s, g_r, x_s, x_r, s0_s, s0_r, s1_s, s1_r, s2_s, s2_r,
):
    e = lax.axis_index("ep")
    t = lax.axis_index("tp")
    z = lax.div(e, 8)
    x = lax.rem(lax.div(e, 2), 4)
    c = lax.rem(e, 2)

    def dev(dz=0, dx=0, flip=False, dy=0):
        cc = 1 - c if flip else c
        return {
            "ep": (up(z, dz, NZ) * NX + up(x, dx, NX)) * NC + cc,
            "tp": up(t, dy, NY),
        }

    def remote(src, dst, ssem, rsem, to):
        return pltpu.make_async_remote_copy(
            src_ref=src, dst_ref=dst, send_sem=ssem, recv_sem=rsem, device_id=to, device_id_type=MESH
        )

    loads = [
        pltpu.make_async_copy(ed_h, ed, lsem.at[0]),
        pltpu.make_async_copy(wo_h, wo, lsem.at[1]),
        pltpu.make_async_copy(eg_h, we.at[:, pl.ds(0, FF)], lsem.at[2]),
        pltpu.make_async_copy(eu_h, we.at[:, pl.ds(FF, FF)], lsem.at[3]),
        pltpu.make_async_copy(dg_h, wd.at[:, pl.ds(0, FF)], lsem.at[4]),
        pltpu.make_async_copy(du_h, wd.at[:, pl.ds(FF, FF)], lsem.at[5]),
        pltpu.make_async_copy(dd_h.at[:, pl.ds(pl.multiple_of(t * Q, Q), Q)], dd, lsem.at[6]),
    ]
    for load in loads:
        load.start()

    barrier = pltpu.get_barrier_semaphore()
    peers = (
        [dev(dy=k) for k in (1, 2, 3)]
        + [dev(dx=k) for k in (1, 2, 3)]
        + [dev(dz=k) for k in range(1, 8)]
        + [dev(flip=True)]
    )
    for peer in peers:
        pl.semaphore_signal(barrier, inc=1, device_id=peer, device_id_type=MESH)

    ids_f = ids_t[...].astype(F32)
    rw = rw_t[...]
    row16 = lax.broadcasted_iota(jnp.int32, (SEQ, SEQ), 0)
    col16 = lax.broadcasted_iota(jnp.int32, (SEQ, SEQ), 1)
    eye = row16 == col16

    def column(rows, k):
        spread = jnp.broadcast_to(rows[k : k + 1, :], (SEQ, SEQ))
        return jnp.sum(jnp.where(eye, spread, 0.0), axis=1, keepdims=True)

    lane = lax.broadcasted_iota(jnp.int32, (SEQ, INFO), 1)
    lane_f = lane.astype(F32)
    id_cols = [column(ids_f, k) for k in (0, 1)]
    w_cols = [column(rw, k) for k in (0, 1)]
    member = jnp.where(lane_f == id_cols[0], 1.0, 0.0) + jnp.where(lane_f == id_cols[1], 1.0, 0.0)
    before = jnp.where(row16 > col16, 1.0, 0.0).astype(BF16)
    earlier = dot(before, member.astype(BF16))

    def split3(v):
        hi = v.astype(BF16).astype(F32)
        rest = v - hi
        mid = rest.astype(BF16).astype(F32)
        return [hi, mid, rest - mid]

    fields = list(id_cols)
    for k in (0, 1):
        fields.append(
            jnp.sum(jnp.where(lane_f == id_cols[k], earlier, 0.0), axis=1, keepdims=True)
        )
    fields += split3(w_cols[0]) + split3(w_cols[1])
    info = jnp.zeros((SEQ, INFO), F32)
    for i, field in enumerate(fields):
        info = jnp.where(lane == i, field, info)

    pl.semaphore_wait(barrier, 14)

    heads_out = [
        remote(heads, hg.at[t], h_s.at[k - 1], h_r.at[k - 1], dev(dy=k)) for k in (1, 2, 3)
    ]
    for copy in heads_out:
        copy.start()
    loads[0].wait()
    ed_out = []
    for k in (1, 2, 3):
        cols = pl.ds(pl.multiple_of(up(t, k, NY) * Q, Q), Q)
        copy = remote(ed.at[:, cols], edx.at[t], ed_s.at[k - 1], ed_r.at[k - 1], dev(dy=k))
        copy.start()
        ed_out.append(copy)
    own_cols = pl.ds(pl.multiple_of(t * Q, Q), Q)
    loads[1].wait()

    def wo_rows(src):
        return wo[pl.ds(pl.multiple_of(src * Q, Q), Q), :]

    total = resid[:, own_cols].astype(F32) + dot(heads[...], wo_rows(t))
    for k in (1, 3, 2):
        src = up(t, -k, NY)
        remote(heads, hg.at[src], h_s.at[k - 1], h_r.at[k - 1], dev()).wait_recv()
        total = total + dot(hg[src], wo_rows(src))
    stream_cols = total.astype(BF16)
    sg[t] = stream_cols
    cols_out = [
        remote(sg.at[t], sg.at[t], c_s.at[k - 1], c_r.at[k - 1], dev(dy=k)) for k in (1, 2, 3)
    ]
    for copy in cols_out:
        copy.start()
    for k in (1, 3, 2):
        src = up(t, -k, NY)
        remote(sg.at[src], sg.at[src], c_s.at[k - 1], c_r.at[k - 1], dev()).wait_recv()
    stream = jnp.concatenate([sg[k] for k in range(NY)], axis=1).astype(F32)
    ffn_in = rms_rows(stream, gain[...]).astype(BF16)
    mix = jax.nn.sigmoid(jnp.sum(ffn_in.astype(F32) * mix_w[...], axis=-1, keepdims=True))
    for i, field in enumerate(split3(mix)):
        info = jnp.where(lane == 10 + i, field, info)
    xg[x, c, z, :, 0:D] = ffn_in
    xg[x, c, z, :, D:WIDE] = info.astype(BF16)

    counter = [0]

    def send(px, pc, pz, **to):
        i = counter[0]
        counter[0] += 1
        remote(xg.at[px, pc, pz], xg.at[px, pc, pz], g_s.at[i], g_r.at[px, pc, pz], dev(**to)).start()

    def arrive(px, pc, pz):
        ref = xg.at[px, pc, pz]
        remote(ref, ref, g_s.at[0], g_r.at[px, pc, pz], dev()).wait_recv()

    @pl.when(c == 0)
    def _():
        counter[0] = 0
        for k in (1, 3, 2):
            send(x, 0, z, dx=k)
        send(x, 0, z, dz=1)
        send(x, 0, z, dz=-1)
        send(x, 0, z, flip=True)
        for k in (1, 3, 2):
            px = up(x, k, NX)
            arrive(px, 0, z)
            send(px, 0, z, dz=1)
            send(px, 0, z, dz=-1)
            send(px, 0, z, flip=True)
        for step in (1, 2, 3):
            for j, k in enumerate(X_ORDER):
                px = up(x, k, NX)
                for sign in (1, -1):
                    pz = up(z, -sign * step, NZ)
                    arrive(px, 0, pz)
                    if step < 3 or (j < 2) == (sign == 1):
                        send(px, 0, pz, dz=sign)
                    send(px, 0, pz, flip=True)
        for k in X_ORDER:
            px = up(x, k, NX)
            pz = up(z, 4, NZ)
            arrive(px, 0, pz)
            send(px, 0, pz, flip=True)
        assert counter[0] == N_SENDS

    @pl.when(c == 1)
    def _():
        counter[0] = 0
        z_order = [0, -1, 1, -2, 2, -3, 3, 4]
        for m, k in enumerate(z_order):
            pz = up(z, k, NZ)
            if m:
                arrive(x, 1, pz)
            if m == 0:
                send(x, 1, pz, dz=1)
                send(x, 1, pz, dz=-1)
            elif k < 0:
                send(x, 1, pz, dz=1)
            elif k < 3:
                send(x, 1, pz, dz=-1)
            send(x, 1, pz, dx=1)
            send(x, 1, pz, dx=-1)
            send(x, 1, pz, flip=True)
        for m, k in enumerate(z_order):
            pz = up(z, k, NZ)
            for sign in (1, -1):
                px = up(x, -sign, NX)
                arrive(px, 1, pz)
                if (m % 2 == 0) == (sign == 1):
                    send(px, 1, pz, dx=sign)
                send(px, 1, pz, flip=True)
        for k in z_order:
            px = up(x, 2, NX)
            pz = up(z, k, NZ)
            arrive(px, 1, pz)
            send(px, 1, pz, flip=True)
        assert counter[0] == N_SENDS

    def sibling_arrival(i, carry):
        arrive(lax.div(i, NZ), 1 - c, lax.rem(i, NZ))
        return carry

    lax.fori_loop(0, NX * NZ, sibling_arrival, 0)

    for load in loads[2:]:
        load.wait()
    e_f = e.astype(F32)
    brow = lax.broadcasted_iota(jnp.int32, (INFO, INFO), 0)
    spans = ((0, 1), (1, 2), (2, 3), (3, 4), (4, 7), (7, 10), (10, 13))
    spread = jnp.concatenate(
        [jnp.where((brow >= lo) & (brow < hi), 1.0, 0.0).astype(BF16) for lo, hi in spans], axis=1
    )
    rows = NC * NZ * SEQ
    rr = lax.broadcasted_iota(jnp.int32, (rows, INFO), 0)
    ll = lax.broadcasted_iota(jnp.int32, (rows, INFO), 1)
    rel = (ll - 2 * lax.div(rr, SEQ)).astype(F32)

    def expert_rows(i, carry):
        block = xg[i].reshape(rows, WIDE)
        both = dot(block[:, 0:D], we[...])
        hidden = (jax.nn.silu(both[:, 0:FF]) * both[:, FF:]).astype(BF16)
        b = dot(block[:, D:WIDE], spread)
        part = [b[:, k * INFO : (k + 1) * INFO] for k in range(7)]
        m0 = part[0] == e_f
        m1 = part[1] == e_f
        wc[i] = jnp.where(m0, part[4], 0.0) + jnp.where(m1, part[5], 0.0)
        mc[i] = part[6]
        slot = jnp.where(m0, part[2], jnp.where(m1, part[3], -4096.0))
        base = (i * (2 * NC * NZ)).astype(F32)
        chosen = jnp.where(slot == rel - base, 1.0, 0.0).astype(BF16)
        st[i] = chosen
        he[...] = hidden
        got = lax.dot_general(
            st[i], he[...], (((0,), (0,)), ((), ())), preferred_element_type=F32
        )

        @pl.when(i == 0)
        def _():
            slots[...] = got

        @pl.when(i > 0)
        def _():
            slots[...] += got

        return carry

    lax.fori_loop(0, NX, expert_rows, 0)
    hx[t] = slots[...].astype(BF16)
    hid_out = [
        remote(hx.at[t], hx.at[t], x_s.at[k - 1], x_r.at[k - 1], dev(dy=k)) for k in (1, 2, 3)
    ]
    for copy in hid_out:
        copy.start()

    def dense_rows(i, carry):
        block = xg[i].reshape(rows, WIDE)
        both = dot(block[:, 0:D], wd[...])
        hd[i] = (jax.nn.silu(both[:, 0:FF]) * both[:, FF:]).astype(BF16)
        return carry

    lax.fori_loop(0, NX, dense_rows, 0)

    edx[t] = ed[:, own_cols]
    for k in (1, 3, 2):
        src = up(t, -k, NY)
        remote(edx.at[src], edx.at[src], ed_s.at[k - 1], ed_r.at[k - 1], dev()).wait_recv()
        remote(hx.at[src], hx.at[src], x_s.at[k - 1], x_r.at[k - 1], dev()).wait_recv()
    result = jnp.zeros((2 * NX * NC * NZ, Q), F32)
    for k in range(NY):
        result = result + dot(hx[k], edx[k]).astype(BF16).astype(F32)
    eo[...] = result.astype(BF16)

    half = NZ * SEQ

    def part_of(px, pc):
        at = pl.ds(pl.multiple_of(pc * half, half), half)
        four = lambda a: jnp.concatenate([a] * 4, axis=1)
        dense = dot(hd[px, at, :], dd[...])
        routed = dot(st[px, at, :], eo[...])
        return four(mc[px, at, :]) * dense + four(wc[px, at, :]) * routed

    x_seq = (2, 1, 3, 0)
    pair_out = {}
    for k in x_seq:
        px = up(x, k, NX)
        s0[k] = part_of(px, 1 - c).astype(BF16)
        pair_out[k] = remote(s0.at[k], r0.at[k], s0_s.at[k], s0_r.at[k], dev(flip=True))
        pair_out[k].start()
        own[k] = part_of(px, c)
    x_out = {}
    for k in x_seq:
        pair_out[k].wait_recv()
        joined = own[k] + r0[k].astype(F32)
        if k:
            s1[k - 1] = joined.astype(BF16)
            x_out[k] = remote(s1.at[k - 1], r1.at[k - 1], s1_s.at[k - 1], s1_r.at[k - 1], dev(dx=k))
            x_out[k].start()
        else:
            own[0] = joined
    sums = own[0]
    for k in (1, 3, 2):
        x_out[k].wait_recv()
        sums = sums + r1[k - 1].astype(F32)
    bsum[...] = sums.reshape(NZ, SEQ, Q)
    s2[...] = sums.astype(BF16).reshape(NZ, SEQ, Q)
    z_out = []
    for k in (4, 3, 5, 2, 6, 1, 7):
        pz = up(z, k, NZ)
        copy = remote(s2.at[pz], r2.at[k - 1], s2_s.at[k - 1], s2_r.at[k - 1], dev(dz=k))
        copy.start()
        z_out.append(copy)
    final = stream_cols.astype(F32) + bsum[z]
    for copy in reversed(z_out):
        copy.wait_recv()
    for k in range(NZ - 1):
        final = final + r2[k].astype(F32)
    out[...] = final

    for copy in heads_out + ed_out + cols_out + hid_out + list(pair_out.values()):
        copy.wait_send()
    for copy in list(x_out.values()) + z_out:
        copy.wait_send()

    def sent(i, carry):
        ref = xg.at[0, 0, 0]
        remote(ref, ref, g_s.at[i], g_r.at[0, 0, 0], dev()).wait_send()
        return carry

    lax.fori_loop(0, N_SENDS, sent, 0)


def tail(*operands):
    vmem = pl.BlockSpec(memory_space=pltpu.VMEM)
    hbm = pl.BlockSpec(memory_space=pl.ANY)
    rows = NC * NZ * SEQ
    dma = lambda *n: pltpu.SemaphoreType.DMA(n)
    buf = lambda shape, kind=BF16: pltpu.VMEM(shape, kind)
    return pl.pallas_call(
        tail_kernel,
        out_shape=jax.ShapeDtypeStruct((SEQ, Q), F32),
        in_specs=[vmem] * 6 + [hbm] * 7,
        out_specs=vmem,
        scratch_shapes=[
            buf((D, Q)),
            buf((D, 2 * FF)),
            buf((D, 2 * FF)),
            buf((FF, D)),
            buf((FF, Q)),
            buf((NY, FF, Q)),
            buf((NY, SEQ, Q)),
            buf((NY, SEQ, Q)),
            buf((NX, NC, NZ, SEQ, WIDE)),
            buf((rows, FF)),
            buf((NX, rows, FF)),
            buf((NX, rows, INFO)),
            buf((NX, rows, INFO), F32),
            buf((NX, rows, INFO), F32),
            buf((NY, 128, FF)),
            buf((128, FF), F32),
            buf((128, Q)),
            buf((NX, NZ * SEQ, Q)),
            buf((NX, NZ * SEQ, Q)),
            buf((NX, NZ * SEQ, Q), F32),
            buf((NX - 1, NZ * SEQ, Q)),
            buf((NX - 1, NZ * SEQ, Q)),
            buf((NZ, SEQ, Q), F32),
            buf((NZ, SEQ, Q)),
            buf((NZ - 1, SEQ, Q)),
            dma(7),
            dma(3), dma(3), dma(3), dma(3), dma(3), dma(3),
            dma(N_SENDS), dma(NX, NC, NZ),
            dma(3), dma(3), dma(4), dma(4), dma(3), dma(3), dma(7), dma(7),
        ],
        compiler_params=pltpu.CompilerParams(
            collective_id=0, has_side_effects=True, vmem_limit_bytes=48 * 1024 * 1024
        ),
        name="tail",
    )(*operands)


def on_device(
    residual_in, lengths, kv_cache, norm_gain_attn, query_weight, key_weight, value_weight,
    diff_lambda, head_gain, out_weight, norm_gain_ffn, route_ids, route_weights, expert_gate,
    expert_up, expert_down, dense_gate, dense_up, dense_down, dense_mix,
):
    seq_count, width = residual_in.shape
    groups = kv_cache.shape[1]
    local_heads = diff_lambda.shape[0]
    resid = residual_in.astype(F32)
    normed = rms_rows(resid, norm_gain_attn).astype(BF16)
    positions = lengths.astype(F32)
    query = dot(normed, query_weight).reshape(seq_count, local_heads, 2, QK_DIM)
    query = rotate(query, positions).astype(BF16)
    keys = dot(normed, key_weight).reshape(seq_count, groups, 2, QK_DIM)
    keys = rotate(keys, positions).astype(BF16).reshape(seq_count, groups, 2 * QK_DIM)
    values = dot(normed, value_weight).reshape(seq_count, groups, HEAD_DIM).astype(BF16)
    fresh = jnp.concatenate([keys, values], axis=-1)
    mixed = attend(query, fresh, kv_cache, lengths, diff_lambda)
    heads_out = rms_rows(mixed, head_gain).astype(BF16).reshape(seq_count, local_heads * HEAD_DIM)
    final = tail(
        heads_out,
        residual_in,
        norm_gain_ffn.reshape(1, width),
        dense_mix.reshape(1, width),
        route_ids.T,
        route_weights.T,
        out_weight,
        expert_gate.reshape(width, -1),
        expert_up.reshape(width, -1),
        expert_down.reshape(-1, width),
        dense_gate,
        dense_up,
        dense_down,
    )
    return (final.astype(BF16), fresh)


def solution(mesh):
    placed = (
        P("ep", None),
        P("ep"),
        P("ep", "tp", None, None),
        P(),
        P(None, "tp"),
        P(None, "tp"),
        P(None, "tp"),
        P("tp"),
        P(),
        P(None, "tp"),
        P(),
        P("ep", None),
        P("ep", None),
        P("ep", None, "tp"),
        P("ep", None, "tp"),
        P("ep", "tp", None),
        P(None, "ep"),
        P(None, "ep"),
        P("ep", None),
        P(),
    )
    return jax.shard_map(
        on_device,
        mesh=mesh,
        in_specs=placed,
        out_specs=(P("ep", "tp"), P("ep", "tp", None)),
        check_vma=False,
    )
```

```python
import jax
import jax.numpy as jnp
import numpy as np
from jax import lax
from jax.experimental import pallas as pl
from jax.experimental.pallas import tpu as pltpu
from jax.sharding import PartitionSpec as P

QK_DIM = 64
HEAD_DIM = 128
EPS = 1e-06
MESH = pl.DeviceIdType.MESH
F32 = jnp.float32
BF16 = jnp.bfloat16
NX, NZ, NY, NC = 4, 8, 4, 2
SEQ = 16
D = 2048
Q = 512
INFO = 128
WIDE = D + INFO
FF = 128
X_ORDER = (0, 1, 3, 2)
N_SENDS = 63


def rms_rows(values, gain):
    mean_sq = jnp.mean(values * values, axis=-1, keepdims=True)
    return values * lax.rsqrt(mean_sq + EPS) * gain


def dot(a, b):
    return jnp.dot(a, b, preferred_element_type=F32)


def up(v, n, size):
    return lax.rem(v + (n % size), size)


def layer_kernel(
    resid_h, lens_h, kv_h, ga_h, wq_h, wk_h, wv_h, lam_h, hgain_h, wo_h, gf_h, ids_h, rw_h,
    eg_h, eu_h, ed_h, dg_h, du_h, dd_h, mixw_h, inv_h, out, rows_out,
    resid, lens, kv, gain_a, wqkv, lam, hgain, gain, ids_t, rw_t, mix_w, inv,
    qs, fk, fv, lenb, mixed, heads,
    wo, we, wd, ed, dd, edx, hg, sg, xg, he, hd, st, wc, mc, hx, slots, eo,
    s0, r0, own, s1, r1, bsum, s2, r2,
    lsem, ed_s, ed_r, h_s, h_r, c_s, c_r, g_s, g_r, x_s, x_r, s0_s, s0_r, s1_s, s1_r, s2_s, s2_r,
):
    e = lax.axis_index("ep")
    t = lax.axis_index("tp")
    z = lax.div(e, 8)
    x = lax.rem(lax.div(e, 2), 4)
    c = lax.rem(e, 2)

    def dev(dz=0, dx=0, flip=False, dy=0):
        cc = 1 - c if flip else c
        return {
            "ep": (up(z, dz, NZ) * NX + up(x, dx, NX)) * NC + cc,
            "tp": up(t, dy, NY),
        }

    def remote(src, dst, ssem, rsem, to):
        return pltpu.make_async_remote_copy(
            src_ref=src, dst_ref=dst, send_sem=ssem, recv_sem=rsem, device_id=to, device_id_type=MESH
        )

    pairs = [
        (lens_h, lens), (ids_h, ids_t), (rw_h, rw_t), (inv_h, inv), (resid_h, resid), (ga_h, gain_a),
        (wq_h, wqkv.at[:, pl.ds(0, Q)]),
        (wk_h, wqkv.at[:, pl.ds(Q, HEAD_DIM)]),
        (wv_h, wqkv.at[:, pl.ds(Q + HEAD_DIM, HEAD_DIM)]),
        (lam_h, lam), (hgain_h, hgain),
    ]
    pairs += [(kv_h.at[pl.ds(4 * g, 4)], kv.at[pl.ds(4 * g, 4)]) for g in range(4)]
    pairs += [
        (wo_h, wo), (gf_h, gain), (mixw_h, mix_w), (ed_h, ed),
        (eg_h, we.at[:, pl.ds(0, FF)]), (eu_h, we.at[:, pl.ds(FF, FF)]),
        (dg_h, wd.at[:, pl.ds(0, FF)]), (du_h, wd.at[:, pl.ds(FF, FF)]),
        (dd_h.at[:, pl.ds(pl.multiple_of(t * Q, Q), Q)], dd),
    ]
    loads = [pltpu.make_async_copy(a, b, lsem.at[i]) for i, (a, b) in enumerate(pairs)]
    for load in loads:
        load.start()
    KV0 = 11
    WO = KV0 + 4

    barrier = pltpu.get_barrier_semaphore()
    peers = (
        [dev(dy=k) for k in (1, 2, 3)]
        + [dev(dx=k) for k in (1, 2, 3)]
        + [dev(dz=k) for k in range(1, 8)]
        + [dev(flip=True)]
    )
    for peer in peers:
        pl.semaphore_signal(barrier, inc=1, device_id=peer, device_id_type=MESH)

    for load in loads[:4]:
        load.wait()

    ids_f = ids_t[...].astype(F32)
    rw = rw_t[...]
    row16 = lax.broadcasted_iota(jnp.int32, (SEQ, SEQ), 0)
    col16 = lax.broadcasted_iota(jnp.int32, (SEQ, SEQ), 1)
    eye = row16 == col16

    def column(rows, k):
        spread = jnp.broadcast_to(rows[k : k + 1, :], (SEQ, SEQ))
        return jnp.sum(jnp.where(eye, spread, 0.0), axis=1, keepdims=True)

    lane = lax.broadcasted_iota(jnp.int32, (SEQ, INFO), 1)
    lane_f = lane.astype(F32)
    id_cols = [column(ids_f, k) for k in (0, 1)]
    w_cols = [column(rw, k) for k in (0, 1)]
    member = jnp.where(lane_f == id_cols[0], 1.0, 0.0) + jnp.where(lane_f == id_cols[1], 1.0, 0.0)
    before = jnp.where(row16 > col16, 1.0, 0.0).astype(BF16)
    earlier = dot(before, member.astype(BF16))

    def split3(v):
        hi = v.astype(BF16).astype(F32)
        rest = v - hi
        mid = rest.astype(BF16).astype(F32)
        return [hi, mid, rest - mid]

    fields = list(id_cols)
    for k in (0, 1):
        fields.append(
            jnp.sum(jnp.where(lane_f == id_cols[k], earlier, 0.0), axis=1, keepdims=True)
        )
    fields += split3(w_cols[0]) + split3(w_cols[1])
    info = jnp.zeros((SEQ, INFO), F32)
    for i, field in enumerate(fields):
        info = jnp.where(lane == i, field, info)

    lane1 = lax.broadcasted_iota(jnp.int32, (SEQ, HEAD_DIM), 1)
    length = column(lens[...].astype(F32), 0)
    lenb[...] = jnp.broadcast_to(length, (SEQ, HEAD_DIM))
    angle = length * inv[...]
    cosine = jnp.cos(angle)
    low = lax.rem(lane1, QK_DIM) < QK_DIM // 2
    sine = jnp.where(low, -jnp.sin(angle), jnp.sin(angle))

    def turned(v):
        ahead = pltpu.roll(v, HEAD_DIM - QK_DIM // 2, 1)
        behind = pltpu.roll(v, QK_DIM // 2, 1)
        return (v * cosine + jnp.where(low, ahead, behind) * sine).astype(BF16)

    for load in loads[4:6]:
        load.wait()
    normed = rms_rows(resid[...].astype(F32), gain_a[...]).astype(BF16)
    for load in loads[6:KV0]:
        load.wait()
    proj = dot(normed, wqkv[...])
    key_new = turned(proj[:, Q : Q + HEAD_DIM])
    val_new = proj[:, Q + HEAD_DIM :].astype(BF16)
    rows_out[:, 0:HEAD_DIM] = key_new
    rows_out[:, HEAD_DIM:] = val_new
    fk[...] = key_new.astype(F32)
    fv[...] = val_new.astype(F32)
    first = lane1 < QK_DIM
    turned_q = [turned(proj[:, j * HEAD_DIM : (j + 1) * HEAD_DIM]) for j in range(4)]
    zero = jnp.zeros((SEQ, HEAD_DIM), BF16)
    stack = jnp.concatenate(
        [jnp.where(first, q, zero) for q in turned_q] + [jnp.where(first, zero, q) for q in turned_q],
        axis=0,
    )
    prow = lax.broadcasted_iota(jnp.int32, (128, 128), 0)
    pcol = lax.broadcasted_iota(jnp.int32, (128, 128), 1)
    to_seq = lax.rem(prow, 8) * SEQ + lax.div(prow, 8) == pcol
    to_head = lax.rem(prow, SEQ) * 8 + lax.div(prow, SEQ) == pcol
    qs[...] = dot(jnp.where(to_seq, 1.0, 0.0).astype(BF16), stack).reshape(SEQ, 8, HEAD_DIM)

    srow = lax.broadcasted_iota(jnp.int32, (8, 4), 0)
    scol = lax.broadcasted_iota(jnp.int32, (8, 4), 1)
    lam_col = jnp.sum(
        jnp.where(srow - 4 == scol, jnp.broadcast_to(lam[...], (8, 4)), 0.0), axis=1, keepdims=True
    )
    sign = jnp.where(lax.broadcasted_iota(jnp.int32, (8, 1), 0) < 4, 1.0, -lam_col)
    position = lax.broadcasted_iota(jnp.int32, (8, 512), 1).astype(F32)
    scale = QK_DIM ** (-0.5)

    def four_sequences(g, carry):
        pltpu.make_async_copy(
            kv_h.at[pl.ds(4 * g, 4)], kv.at[pl.ds(4 * g, 4)], lsem.at[KV0 + g]
        ).wait()
        for i in range(4):
            b = 4 * g + i
            qb = qs[b]
            scores = scale * lax.dot_general(
                qb.astype(BF16), kv[b, :, 0:HEAD_DIM], (((1,), (1,)), ((), ())),
                preferred_element_type=F32,
            )
            latest = scale * jnp.sum(qb * fk[pl.ds(b, 1), :], axis=1, keepdims=True)
            valid = position < lenb[pl.ds(b, 1), 0:1]
            masked = jnp.where(valid, scores, -1e30)
            top = jnp.maximum(jnp.max(masked, axis=1, keepdims=True), latest)
            raised = jnp.where(valid, jnp.exp(masked - top), 0.0)
            raised_new = jnp.exp(latest - top)
            weight = sign / (jnp.sum(raised, axis=1, keepdims=True) + raised_new)
            both = raised * weight
            mapped = (both + pltpu.roll(both, 4, 0)).astype(BF16)
            new = raised_new * weight
            mapped_new = (new + pltpu.roll(jnp.broadcast_to(new, (8, HEAD_DIM)), 4, 0)).astype(BF16)
            mixed[b] = dot(mapped, kv[b, :, HEAD_DIM:]) + mapped_new.astype(F32) * fv[pl.ds(b, 1), :]
        return carry

    lax.fori_loop(0, 4, four_sequences, 0)
    normed_heads = rms_rows(mixed[...].reshape(128, HEAD_DIM), hgain[...]).astype(BF16)
    by_head = dot(jnp.where(to_head, 1.0, 0.0).astype(BF16), normed_heads).astype(BF16)
    for j in range(4):
        heads[:, j * HEAD_DIM : (j + 1) * HEAD_DIM] = by_head[j * SEQ : (j + 1) * SEQ, :]

    pl.semaphore_wait(barrier, 14)

    heads_out = [
        remote(heads, hg.at[t], h_s.at[k - 1], h_r.at[k - 1], dev(dy=k)) for k in (1, 2, 3)
    ]
    for copy in heads_out:
        copy.start()
    own_cols = pl.ds(pl.multiple_of(t * Q, Q), Q)
    for load in loads[WO:WO + 4]:
        load.wait()

    def wo_rows(src):
        return wo[pl.ds(pl.multiple_of(src * Q, Q), Q), :]

    total = resid[:, own_cols].astype(F32) + dot(heads[...], wo_rows(t))
    for k in (1, 3, 2):
        src = up(t, -k, NY)
        remote(heads, hg.at[src], h_s.at[k - 1], h_r.at[k - 1], dev()).wait_recv()
        total = total + dot(hg[src], wo_rows(src))
    stream_cols = total.astype(BF16)
    sg[t] = stream_cols
    cols_out = [
        remote(sg.at[t], sg.at[t], c_s.at[k - 1], c_r.at[k - 1], dev(dy=k)) for k in (1, 2, 3)
    ]
    for copy in cols_out:
        copy.start()
    ed_out = []
    for k in (1, 2, 3):
        cols = pl.ds(pl.multiple_of(up(t, k, NY) * Q, Q), Q)
        copy = remote(ed.at[:, cols], edx.at[t], ed_s.at[k - 1], ed_r.at[k - 1], dev(dy=k))
        copy.start()
        ed_out.append(copy)
    for k in (1, 3, 2):
        src = up(t, -k, NY)
        remote(sg.at[src], sg.at[src], c_s.at[k - 1], c_r.at[k - 1], dev()).wait_recv()
    stream = jnp.concatenate([sg[k] for k in range(NY)], axis=1).astype(F32)
    ffn_in = rms_rows(stream, gain[...]).astype(BF16)
    mix = jax.nn.sigmoid(jnp.sum(ffn_in.astype(F32) * mix_w[...], axis=-1, keepdims=True))
    for i, field in enumerate(split3(mix)):
        info = jnp.where(lane == 10 + i, field, info)
    xg[x, c, z, :, 0:D] = ffn_in
    xg[x, c, z, :, D:WIDE] = info.astype(BF16)

    counter = [0]

    def send(px, pc, pz, **to):
        i = counter[0]
        counter[0] += 1
        remote(xg.at[px, pc, pz], xg.at[px, pc, pz], g_s.at[i], g_r.at[px, pc, pz], dev(**to)).start()

    def arrive(px, pc, pz):
        ref = xg.at[px, pc, pz]
        remote(ref, ref, g_s.at[0], g_r.at[px, pc, pz], dev()).wait_recv()

    @pl.when(c == 0)
    def _():
        counter[0] = 0
        for k in (1, 3, 2):
            send(x, 0, z, dx=k)
        send(x, 0, z, dz=1)
        send(x, 0, z, dz=-1)
        send(x, 0, z, flip=True)
        for k in (1, 3, 2):
            px = up(x, k, NX)
            arrive(px, 0, z)
            send(px, 0, z, dz=1)
            send(px, 0, z, dz=-1)
            send(px, 0, z, flip=True)
        for step in (1, 2, 3):
            for j, k in enumerate(X_ORDER):
                px = up(x, k, NX)
                for sign in (1, -1):
                    pz = up(z, -sign * step, NZ)
                    arrive(px, 0, pz)
                    if step < 3 or (j < 2) == (sign == 1):
                        send(px, 0, pz, dz=sign)
                    send(px, 0, pz, flip=True)
        for k in X_ORDER:
            px = up(x, k, NX)
            pz = up(z, 4, NZ)
            arrive(px, 0, pz)
            send(px, 0, pz, flip=True)
        assert counter[0] == N_SENDS

    @pl.when(c == 1)
    def _():
        counter[0] = 0
        z_order = [0, -1, 1, -2, 2, -3, 3, 4]
        for m, k in enumerate(z_order):
            pz = up(z, k, NZ)
            if m:
                arrive(x, 1, pz)
            if m == 0:
                send(x, 1, pz, dz=1)
                send(x, 1, pz, dz=-1)
            elif k < 0:
                send(x, 1, pz, dz=1)
            elif k < 3:
                send(x, 1, pz, dz=-1)
            send(x, 1, pz, dx=1)
            send(x, 1, pz, dx=-1)
            send(x, 1, pz, flip=True)
        for m, k in enumerate(z_order):
            pz = up(z, k, NZ)
            for sign in (1, -1):
                px = up(x, -sign, NX)
                arrive(px, 1, pz)
                if (m % 2 == 0) == (sign == 1):
                    send(px, 1, pz, dx=sign)
                send(px, 1, pz, flip=True)
        for k in z_order:
            px = up(x, 2, NX)
            pz = up(z, k, NZ)
            arrive(px, 1, pz)
            send(px, 1, pz, flip=True)
        assert counter[0] == N_SENDS

    def sibling_arrival(i, carry):
        arrive(lax.div(i, NZ), 1 - c, lax.rem(i, NZ))
        return carry

    lax.fori_loop(0, NX * NZ, sibling_arrival, 0)

    for load in loads[WO + 4:]:
        load.wait()
    e_f = e.astype(F32)
    brow = lax.broadcasted_iota(jnp.int32, (INFO, INFO), 0)
    spans = ((0, 1), (1, 2), (2, 3), (3, 4), (4, 7), (7, 10), (10, 13))
    spread = jnp.concatenate(
        [jnp.where((brow >= lo) & (brow < hi), 1.0, 0.0).astype(BF16) for lo, hi in spans], axis=1
    )
    rows = NC * NZ * SEQ
    rr = lax.broadcasted_iota(jnp.int32, (rows, INFO), 0)
    ll = lax.broadcasted_iota(jnp.int32, (rows, INFO), 1)
    rel = (ll - 2 * lax.div(rr, SEQ)).astype(F32)

    def expert_rows(i, carry):
        block = xg[i].reshape(rows, WIDE)
        both = dot(block[:, 0:D], we[...])
        hidden = (jax.nn.silu(both[:, 0:FF]) * both[:, FF:]).astype(BF16)
        b = dot(block[:, D:WIDE], spread)
        part = [b[:, k * INFO : (k + 1) * INFO] for k in range(7)]
        m0 = part[0] == e_f
        m1 = part[1] == e_f
        wc[i] = jnp.where(m0, part[4], 0.0) + jnp.where(m1, part[5], 0.0)
        mc[i] = part[6]
        slot = jnp.where(m0, part[2], jnp.where(m1, part[3], -4096.0))
        base = (i * (2 * NC * NZ)).astype(F32)
        chosen = jnp.where(slot == rel - base, 1.0, 0.0).astype(BF16)
        st[i] = chosen
        he[...] = hidden
        got = lax.dot_general(
            st[i], he[...], (((0,), (0,)), ((), ())), preferred_element_type=F32
        )

        @pl.when(i == 0)
        def _():
            slots[...] = got

        @pl.when(i > 0)
        def _():
            slots[...] += got

        return carry

    lax.fori_loop(0, NX, expert_rows, 0)
    hx[t] = slots[...].astype(BF16)
    hid_out = [
        remote(hx.at[t], hx.at[t], x_s.at[k - 1], x_r.at[k - 1], dev(dy=k)) for k in (1, 2, 3)
    ]
    for copy in hid_out:
        copy.start()

    def dense_rows(i, carry):
        block = xg[i].reshape(rows, WIDE)
        both = dot(block[:, 0:D], wd[...])
        hd[i] = (jax.nn.silu(both[:, 0:FF]) * both[:, FF:]).astype(BF16)
        return carry

    lax.fori_loop(0, NX, dense_rows, 0)

    edx[t] = ed[:, own_cols]
    for k in (1, 3, 2):
        src = up(t, -k, NY)
        remote(edx.at[src], edx.at[src], ed_s.at[k - 1], ed_r.at[k - 1], dev()).wait_recv()
        remote(hx.at[src], hx.at[src], x_s.at[k - 1], x_r.at[k - 1], dev()).wait_recv()
    result = jnp.zeros((2 * NX * NC * NZ, Q), F32)
    for k in range(NY):
        result = result + dot(hx[k], edx[k]).astype(BF16).astype(F32)
    eo[...] = result.astype(BF16)

    half = NZ * SEQ

    def part_of(px, pc):
        at = pl.ds(pl.multiple_of(pc * half, half), half)
        four = lambda a: jnp.concatenate([a] * 4, axis=1)
        dense = dot(hd[px, at, :], dd[...])
        routed = dot(st[px, at, :], eo[...])
        return four(mc[px, at, :]) * dense + four(wc[px, at, :]) * routed

    x_seq = (2, 1, 3, 0)
    pair_out = {}
    for k in x_seq:
        px = up(x, k, NX)
        s0[k] = part_of(px, 1 - c).astype(BF16)
        pair_out[k] = remote(s0.at[k], r0.at[k], s0_s.at[k], s0_r.at[k], dev(flip=True))
        pair_out[k].start()
        own[k] = part_of(px, c)
    x_out = {}
    for k in x_seq:
        pair_out[k].wait_recv()
        joined = own[k] + r0[k].astype(F32)
        if k:
            s1[k - 1] = joined.astype(BF16)
            x_out[k] = remote(s1.at[k - 1], r1.at[k - 1], s1_s.at[k - 1], s1_r.at[k - 1], dev(dx=k))
            x_out[k].start()
        else:
            own[0] = joined
    sums = own[0]
    for k in (1, 3, 2):
        x_out[k].wait_recv()
        sums = sums + r1[k - 1].astype(F32)
    bsum[...] = sums.reshape(NZ, SEQ, Q)
    s2[...] = sums.astype(BF16).reshape(NZ, SEQ, Q)
    z_out = []
    for k in (4, 3, 5, 2, 6, 1, 7):
        pz = up(z, k, NZ)
        copy = remote(s2.at[pz], r2.at[k - 1], s2_s.at[k - 1], s2_r.at[k - 1], dev(dz=k))
        copy.start()
        z_out.append(copy)
    final = stream_cols.astype(F32) + bsum[z]
    for copy in reversed(z_out):
        copy.wait_recv()
    for k in range(NZ - 1):
        final = final + r2[k].astype(F32)
    out[...] = final

    for copy in heads_out + ed_out + cols_out + hid_out + list(pair_out.values()):
        copy.wait_send()
    for copy in list(x_out.values()) + z_out:
        copy.wait_send()

    def sent(i, carry):
        ref = xg.at[0, 0, 0]
        remote(ref, ref, g_s.at[i], g_r.at[0, 0, 0], dev()).wait_send()
        return carry

    lax.fori_loop(0, N_SENDS, sent, 0)


def layer(*operands):
    vmem = pl.BlockSpec(memory_space=pltpu.VMEM)
    hbm = pl.BlockSpec(memory_space=pltpu.HBM)
    rows = NC * NZ * SEQ
    dma = lambda *n: pltpu.SemaphoreType.DMA(n)
    buf = lambda shape, kind=BF16: pltpu.VMEM(shape, kind)
    return pl.pallas_call(
        layer_kernel,
        out_shape=(
            jax.ShapeDtypeStruct((SEQ, Q), F32),
            jax.ShapeDtypeStruct((SEQ, 2 * HEAD_DIM), BF16),
        ),
        in_specs=[hbm] * len(operands),
        out_specs=(vmem, vmem),
        scratch_shapes=[
            buf((SEQ, D)),
            buf((1, SEQ), jnp.int32),
            buf((SEQ, 512, 2 * HEAD_DIM)),
            buf((1, D), F32),
            buf((D, Q + 2 * HEAD_DIM)),
            buf((1, 4), F32),
            buf((1, HEAD_DIM), F32),
            buf((1, D), F32),
            buf((2, SEQ), jnp.int32),
            buf((2, SEQ), F32),
            buf((1, D), F32),
            buf((1, HEAD_DIM), F32),
            buf((SEQ, 8, HEAD_DIM), F32),
            buf((SEQ, HEAD_DIM), F32),
            buf((SEQ, HEAD_DIM), F32),
            buf((SEQ, HEAD_DIM), F32),
            buf((SEQ, 8, HEAD_DIM), F32),
            buf((SEQ, Q)),
            buf((D, Q)),
            buf((D, 2 * FF)),
            buf((D, 2 * FF)),
            buf((FF, D)),
            buf((FF, Q)),
            buf((NY, FF, Q)),
            buf((NY, SEQ, Q)),
            buf((NY, SEQ, Q)),
            buf((NX, NC, NZ, SEQ, WIDE)),
            buf((rows, FF)),
            buf((NX, rows, FF)),
            buf((NX, rows, INFO)),
            buf((NX, rows, INFO), F32),
            buf((NX, rows, INFO), F32),
            buf((NY, 128, FF)),
            buf((128, FF), F32),
            buf((128, Q)),
            buf((NX, NZ * SEQ, Q)),
            buf((NX, NZ * SEQ, Q)),
            buf((NX, NZ * SEQ, Q), F32),
            buf((NX - 1, NZ * SEQ, Q)),
            buf((NX - 1, NZ * SEQ, Q)),
            buf((NZ, SEQ, Q), F32),
            buf((NZ, SEQ, Q)),
            buf((NZ - 1, SEQ, Q)),
            dma(24),
            dma(3), dma(3), dma(3), dma(3), dma(3), dma(3),
            dma(N_SENDS), dma(NX, NC, NZ),
            dma(3), dma(3), dma(4), dma(4), dma(3), dma(3), dma(7), dma(7),
        ],
        compiler_params=pltpu.CompilerParams(
            collective_id=0, has_side_effects=True, vmem_limit_bytes=60 * 1024 * 1024
        ),
        name="layer",
    )(*operands)


def on_device(
    residual_in, lengths, kv_cache, norm_gain_attn, query_weight, key_weight, value_weight,
    diff_lambda, head_gain, out_weight, norm_gain_ffn, route_ids, route_weights, expert_gate,
    expert_up, expert_down, dense_gate, dense_up, dense_down, dense_mix,
):
    width = residual_in.shape[1]
    half = QK_DIM // 2
    inverse = 10000.0 ** (-np.arange(half, dtype=np.float32) / np.float32(half))
    inverse = np.tile(inverse.astype(np.float32), 4)[None, :]
    final, fresh = layer(
        residual_in,
        lengths.reshape(1, -1),
        kv_cache.reshape(SEQ, 512, 2 * HEAD_DIM),
        norm_gain_attn.reshape(1, width),
        query_weight,
        key_weight,
        value_weight,
        diff_lambda.reshape(1, -1),
        head_gain.reshape(1, -1),
        out_weight,
        norm_gain_ffn.reshape(1, width),
        route_ids.T,
        route_weights.T,
        expert_gate.reshape(width, -1),
        expert_up.reshape(width, -1),
        expert_down.reshape(-1, width),
        dense_gate,
        dense_up,
        dense_down,
        dense_mix.reshape(1, width),
        jnp.asarray(inverse),
    )
    return (final.astype(BF16), fresh.reshape(SEQ, 1, 2 * HEAD_DIM))


def solution(mesh):
    placed = (
        P("ep", None),
        P("ep"),
        P("ep", "tp", None, None),
        P(),
        P(None, "tp"),
        P(None, "tp"),
        P(None, "tp"),
        P("tp"),
        P(),
        P(None, "tp"),
        P(),
        P("ep", None),
        P("ep", None),
        P("ep", None, "tp"),
        P("ep", None, "tp"),
        P("ep", "tp", None),
        P(None, "ep"),
        P(None, "ep"),
        P("ep", None),
        P(),
    )
    return jax.shard_map(
        on_device,
        mesh=mesh,
        in_specs=placed,
        out_specs=(P("ep", "tp"), P("ep", "tp", None)),
        check_vma=False,
    )
```

```python
import jax
import jax.numpy as jnp
import numpy as np
from jax import lax
from jax.experimental import pallas as pl
from jax.experimental.pallas import tpu as pltpu
from jax.sharding import PartitionSpec as P

QK_DIM = 64
HEAD_DIM = 128
EPS = 1e-06
MESH = pl.DeviceIdType.MESH
F32 = jnp.float32
BF16 = jnp.bfloat16
NX, NZ, NY, NC = 4, 8, 4, 2
SEQ = 16
D = 2048
Q = 512
INFO = 128
WIDE = D + INFO
FF = 128
X_ORDER = (0, 1, 3, 2)
Z_ORDER = (0, -1, 1, -2, 2, -3, 3, 4)
N_SENDS = 67
NOT_SENT = tuple(15 + 32 + 4 * j + (2 if j < 2 else 0) for j in range(4))


def rms_rows(values, gain):
    mean_sq = jnp.mean(values * values, axis=-1, keepdims=True)
    return values * lax.rsqrt(mean_sq + EPS) * gain


def dot(a, b):
    return jnp.dot(a, b, preferred_element_type=F32)


def up(v, n, size, dynamic=False):
    return lax.rem(v + (n if dynamic else n % size), size)


def layer_kernel(
    resid_h, lens_h, kv_h, ga_h, wq_h, wk_h, wv_h, lam_h, hgain_h, wo_h, gf_h, ids_h, rw_h,
    eg_h, eu_h, ed_h, dg_h, du_h, dd_h, mixw_h, inv_h, out, rows_out,
    resid, lens, kv, gain_a, wqkv, lam, hgain, gain, ids_t, rw_t, mix_w, inv,
    qs, fk, fv, lenb, mixed, heads,
    wo, w4, spread, ed, dd, edx, hg, sg, xg, hd, st, wc, mc, hx, slots, eo,
    s0, r0, own, s1, r1, bsum, s2, r2,
    lsem, ed_s, ed_r, h_s, h_r, c_s, c_r, g_s, g_r, x_s, x_r, s0_s, s0_r, s1_s, s1_r, s2_s, s2_r,
):
    e = lax.axis_index("ep")
    t = lax.axis_index("tp")
    z = lax.div(e, 8)
    x = lax.rem(lax.div(e, 2), 4)
    c = lax.rem(e, 2)

    def dev(dz=0, dx=0, flip=False, dy=0):
        cc = 1 - c if flip else c
        return {
            "ep": (up(z, dz, NZ) * NX + up(x, dx, NX)) * NC + cc,
            "tp": up(t, dy, NY),
        }

    def remote(src, dst, ssem, rsem, to):
        return pltpu.make_async_remote_copy(
            src_ref=src, dst_ref=dst, send_sem=ssem, recv_sem=rsem, device_id=to, device_id_type=MESH
        )

    pairs = [
        (lens_h, lens), (ids_h, ids_t), (rw_h, rw_t), (inv_h, inv), (resid_h, resid), (ga_h, gain_a),
        (wq_h, wqkv.at[:, pl.ds(0, Q)]),
        (wk_h, wqkv.at[:, pl.ds(Q, HEAD_DIM)]),
        (wv_h, wqkv.at[:, pl.ds(Q + HEAD_DIM, HEAD_DIM)]),
        (lam_h, lam), (hgain_h, hgain),
    ]
    pairs += [(kv_h.at[pl.ds(4 * g, 4)], kv.at[pl.ds(4 * g, 4)]) for g in range(4)]
    pairs += [
        (wo_h, wo), (gf_h, gain), (mixw_h, mix_w), (ed_h, ed),
        (eg_h, w4.at[:, pl.ds(0, FF)]), (eu_h, w4.at[:, pl.ds(FF, FF)]),
        (dg_h, w4.at[:, pl.ds(2 * FF, FF)]), (du_h, w4.at[:, pl.ds(3 * FF, FF)]),
        (dd_h.at[:, pl.ds(pl.multiple_of(t * Q, Q), Q)], dd),
    ]
    loads = [pltpu.make_async_copy(a, b, lsem.at[i]) for i, (a, b) in enumerate(pairs)]
    for load in loads:
        load.start()
    KV0 = 11
    WO = KV0 + 4

    barrier = pltpu.get_barrier_semaphore()
    peers = (
        [dev(dy=k) for k in (1, 2, 3)]
        + [dev(dx=k) for k in (1, 2, 3)]
        + [dev(dz=k) for k in range(1, 8)]
        + [dev(flip=True)]
    )
    for peer in peers:
        pl.semaphore_signal(barrier, inc=1, device_id=peer, device_id_type=MESH)

    for load in loads[:4]:
        load.wait()

    ids_f = ids_t[...].astype(F32)
    rw = rw_t[...]
    row16 = lax.broadcasted_iota(jnp.int32, (SEQ, SEQ), 0)
    col16 = lax.broadcasted_iota(jnp.int32, (SEQ, SEQ), 1)
    eye = row16 == col16

    def column(rows, k):
        spread = jnp.broadcast_to(rows[k : k + 1, :], (SEQ, SEQ))
        return jnp.sum(jnp.where(eye, spread, 0.0), axis=1, keepdims=True)

    lane = lax.broadcasted_iota(jnp.int32, (SEQ, INFO), 1)
    lane_f = lane.astype(F32)
    id_cols = [column(ids_f, k) for k in (0, 1)]
    w_cols = [column(rw, k) for k in (0, 1)]
    member = jnp.where(lane_f == id_cols[0], 1.0, 0.0) + jnp.where(lane_f == id_cols[1], 1.0, 0.0)
    before = jnp.where(row16 > col16, 1.0, 0.0).astype(BF16)
    earlier = dot(before, member.astype(BF16))

    def split3(v):
        hi = v.astype(BF16).astype(F32)
        rest = v - hi
        mid = rest.astype(BF16).astype(F32)
        return [hi, mid, rest - mid]

    fields = list(id_cols)
    for k in (0, 1):
        fields.append(
            jnp.sum(jnp.where(lane_f == id_cols[k], earlier, 0.0), axis=1, keepdims=True)
        )
    fields += split3(w_cols[0]) + split3(w_cols[1])
    info = jnp.zeros((SEQ, INFO), F32)
    for i, field in enumerate(fields):
        info = jnp.where(lane == i, field, info)

    lane1 = lax.broadcasted_iota(jnp.int32, (SEQ, HEAD_DIM), 1)
    length = column(lens[...].astype(F32), 0)
    lenb[...] = jnp.broadcast_to(length, (SEQ, HEAD_DIM))
    angle = length * inv[...]
    cosine = jnp.cos(angle)
    low = lax.rem(lane1, QK_DIM) < QK_DIM // 2
    sine = jnp.where(low, -jnp.sin(angle), jnp.sin(angle))

    def turned(v):
        ahead = pltpu.roll(v, HEAD_DIM - QK_DIM // 2, 1)
        behind = pltpu.roll(v, QK_DIM // 2, 1)
        return (v * cosine + jnp.where(low, ahead, behind) * sine).astype(BF16)

    for load in loads[4:6]:
        load.wait()
    normed = rms_rows(resid[...].astype(F32), gain_a[...]).astype(BF16)
    for load in loads[6:KV0]:
        load.wait()
    proj = dot(normed, wqkv[...])
    key_new = turned(proj[:, Q : Q + HEAD_DIM])
    val_new = proj[:, Q + HEAD_DIM :].astype(BF16)
    rows_out[:, 0:HEAD_DIM] = key_new
    rows_out[:, HEAD_DIM:] = val_new
    fk[...] = key_new.astype(F32)
    fv[...] = val_new.astype(F32)
    first = lane1 < QK_DIM
    turned_q = [turned(proj[:, j * HEAD_DIM : (j + 1) * HEAD_DIM]) for j in range(4)]
    zero = jnp.zeros((SEQ, HEAD_DIM), BF16)
    stack = jnp.concatenate(
        [jnp.where(first, q, zero) for q in turned_q] + [jnp.where(first, zero, q) for q in turned_q],
        axis=0,
    )
    prow = lax.broadcasted_iota(jnp.int32, (128, 128), 0)
    pcol = lax.broadcasted_iota(jnp.int32, (128, 128), 1)
    to_seq = lax.rem(prow, 8) * SEQ + lax.div(prow, 8) == pcol
    to_head = lax.rem(prow, SEQ) * 8 + lax.div(prow, SEQ) == pcol
    qs[...] = dot(jnp.where(to_seq, 1.0, 0.0).astype(BF16), stack).reshape(SEQ, 8, HEAD_DIM)

    srow = lax.broadcasted_iota(jnp.int32, (8, 4), 0)
    scol = lax.broadcasted_iota(jnp.int32, (8, 4), 1)
    lam_col = jnp.sum(
        jnp.where(srow - 4 == scol, jnp.broadcast_to(lam[...], (8, 4)), 0.0), axis=1, keepdims=True
    )
    sign = jnp.where(lax.broadcasted_iota(jnp.int32, (8, 1), 0) < 4, 1.0, -lam_col)
    sign4 = jnp.concatenate([sign] * 4, axis=0)
    position = lax.broadcasted_iota(jnp.int32, (32, 512), 1).astype(F32)
    scale = QK_DIM ** (-0.5)
    contract_last = (((1,), (1,)), ((), ()))
    for load in loads[KV0:WO]:
        load.wait()
    for g in range(4):
        seqs = range(4 * g, 4 * g + 4)
        q4 = [qs[b] for b in seqs]
        scores = jnp.concatenate(
            [
                lax.dot_general(
                    q.astype(BF16), kv[b, :, 0:HEAD_DIM], contract_last, preferred_element_type=F32
                )
                for q, b in zip(q4, seqs)
            ],
            axis=0,
        )
        latest = scale * jnp.concatenate(
            [jnp.sum(q * fk[b : b + 1, :], axis=1, keepdims=True) for q, b in zip(q4, seqs)], axis=0
        )
        count = jnp.concatenate([jnp.broadcast_to(lenb[b : b + 1, 0:1], (8, 1)) for b in seqs], axis=0)
        masked = jnp.where(position < count, scores * scale, -1e30)
        top = jnp.maximum(jnp.max(masked, axis=1, keepdims=True), latest)
        raised = jnp.exp(masked - top)
        raised_new = jnp.exp(latest - top)
        weight = sign4 / (jnp.sum(raised, axis=1, keepdims=True) + raised_new)
        both = raised * weight
        mapped = (both + pltpu.roll(both, 28, 0)).astype(BF16)
        new = jnp.broadcast_to(raised_new * weight, (32, HEAD_DIM))
        mapped_new = (new + pltpu.roll(new, 28, 0)).astype(BF16).astype(F32)
        for i, b in enumerate(seqs):
            at = slice(8 * i, 8 * i + 8)
            mixed[b] = dot(mapped[at, :], kv[b, :, HEAD_DIM:]) + mapped_new[at, :] * fv[b : b + 1, :]
    normed_heads = rms_rows(mixed[...].reshape(128, HEAD_DIM), hgain[...]).astype(BF16)
    by_head = dot(jnp.where(to_head, 1.0, 0.0).astype(BF16), normed_heads).astype(BF16)
    for j in range(4):
        heads[:, j * HEAD_DIM : (j + 1) * HEAD_DIM] = by_head[j * SEQ : (j + 1) * SEQ, :]

    pl.semaphore_wait(barrier, 14)

    heads_out = [
        remote(heads, hg.at[t], h_s.at[k - 1], h_r.at[k - 1], dev(dy=k)) for k in (1, 2, 3)
    ]
    for copy in heads_out:
        copy.start()
    own_cols = pl.ds(pl.multiple_of(t * Q, Q), Q)
    for load in loads[WO:WO + 4]:
        load.wait()

    def wo_rows(src):
        return wo[pl.ds(pl.multiple_of(src * Q, Q), Q), :]

    total = resid[:, own_cols].astype(F32) + dot(heads[...], wo_rows(t))
    for k in (1, 3, 2):
        src = up(t, -k, NY)
        remote(heads, hg.at[src], h_s.at[k - 1], h_r.at[k - 1], dev()).wait_recv()
        total = total + dot(hg[src], wo_rows(src))
    stream_cols = total.astype(BF16)
    sg[t] = stream_cols
    cols_out = [
        remote(sg.at[t], sg.at[t], c_s.at[k - 1], c_r.at[k - 1], dev(dy=k)) for k in (1, 2, 3)
    ]
    for copy in cols_out:
        copy.start()
    ed_out = []
    for k in (1, 2, 3):
        cols = pl.ds(pl.multiple_of(up(t, k, NY) * Q, Q), Q)
        copy = remote(ed.at[:, cols], edx.at[t], ed_s.at[k - 1], ed_r.at[k - 1], dev(dy=k))
        copy.start()
        ed_out.append(copy)
    for k in (1, 3, 2):
        src = up(t, -k, NY)
        remote(sg.at[src], sg.at[src], c_s.at[k - 1], c_r.at[k - 1], dev()).wait_recv()
    stream = jnp.concatenate([sg[k] for k in range(NY)], axis=1).astype(F32)
    ffn_in = rms_rows(stream, gain[...]).astype(BF16)
    mix = jax.nn.sigmoid(jnp.sum(ffn_in.astype(F32) * mix_w[...], axis=-1, keepdims=True))
    for i, field in enumerate(split3(mix)):
        info = jnp.where(lane == 10 + i, field, info)
    xg[x, c, z, :, 0:D] = ffn_in
    xg[x, c, z, :, D:WIDE] = info.astype(BF16)

    slots[...] = jnp.zeros_like(slots)
    for load in loads[WO + 4 :]:
        load.wait()
    e_f = e.astype(F32)
    brow = lax.broadcasted_iota(jnp.int32, (INFO, INFO), 0)
    spans = ((0, 1), (1, 2), (2, 3), (3, 4), (4, 7), (7, 10), (10, 13))
    for i, (lo, hi) in enumerate(spans):
        spread[:, i * INFO : (i + 1) * INFO] = jnp.where((brow >= lo) & (brow < hi), 1.0, 0.0).astype(BF16)
    grow = lax.div(lax.broadcasted_iota(jnp.int32, (128, INFO), 0), SEQ)
    glane = lax.broadcasted_iota(jnp.int32, (128, INFO), 1)

    def group(block, base):
        both = dot(block[:, 0:D], w4[...])
        hidden = (jax.nn.silu(both[:, 0:FF]) * both[:, FF : 2 * FF]).astype(BF16)
        dense = (jax.nn.silu(both[:, 2 * FF : 3 * FF]) * both[:, 3 * FF :]).astype(BF16)
        b = dot(block[:, D:WIDE], spread[...])
        part = [b[:, k * INFO : (k + 1) * INFO] for k in range(7)]
        m0 = part[0] == e_f
        m1 = part[1] == e_f
        weight = jnp.where(m0, part[4], 0.0) + jnp.where(m1, part[5], 0.0)
        slot = jnp.where(m0, part[2], jnp.where(m1, part[3], -4096.0))
        chosen = jnp.where(slot == (glane - base).astype(F32), 1.0, 0.0).astype(BF16)
        slots[...] += lax.dot_general(
            chosen, hidden, (((0,), (0,)), ((), ())), preferred_element_type=F32
        )
        return dense, chosen, weight, part[6]

    def z_group(step):
        ahead = up(z, lax.rem(step, 4), NZ, True)
        behind = up(z, NZ - step, NZ, True)
        block = jnp.concatenate(
            [xg[:, 1, ahead].reshape(64, WIDE), xg[:, 1, behind].reshape(64, WIDE)], axis=0
        )
        column_of = jnp.where(grow < 4, ahead, behind)
        base = 2 * NC * NZ * lax.rem(grow, 4) + 2 * NZ + 2 * column_of
        for ref, value in zip((hd, st, wc, mc), group(block, base)):
            ref[:, 1, ahead] = value[0:64].reshape(NX, SEQ, INFO)
            ref[:, 1, behind] = value[64:].reshape(NX, SEQ, INFO)

    def x_group(d):
        px = up(x, d, NX, True)
        base = 2 * NC * NZ * px + 2 * grow
        for ref, value in zip((hd, st, wc, mc), group(xg[px, 0].reshape(128, WIDE), base)):
            ref[px, 0] = value.reshape(NZ, SEQ, INFO)

    def x_rank(i):
        return i + jnp.where(i == 2, 1, 0) - jnp.where(i == 3, 1, 0)

    def send(i, px, pc, pz, **to):
        remote(xg.at[px, pc, pz], xg.at[px, pc, pz], g_s.at[i], g_r.at[px, pc, pz], dev(**to)).start()

    def arrive(px, pc, pz):
        ref = xg.at[px, pc, pz]
        remote(ref, ref, g_s.at[0], g_r.at[px, pc, pz], dev()).wait_recv()

    def z_rank(m):
        far = lax.div(m + 1, 2)
        return lax.rem(jnp.where(lax.rem(m, 2) == 1, NZ - far, far), NZ)

    @pl.when(c == 1)
    def _():
        send(0, x, 1, z, dx=2)
        send(1, x, 1, z, dx=1)
        send(2, x, 1, z, dx=-1)
        send(3, x, 1, z, dz=1)
        send(4, x, 1, z, dz=-1)
        send(5, x, 1, z, flip=True)
        for m, k in enumerate((1, 3, 2)):
            px = up(x, k, NX)
            arrive(px, 1, z)
            send(6 + 3 * m, px, 1, z, dz=1)
            send(7 + 3 * m, px, 1, z, dz=-1)
            send(8 + 3 * m, px, 1, z, flip=True)

        def ring_step(step, carry):
            back = up(z, NZ - step, NZ, True)
            front = up(z, step, NZ, True)
            first = 15 + 16 * (step - 1)

            @pl.when(step < 4)
            def _():
                for j, k in enumerate(X_ORDER):
                    px = up(x, k, NX)
                    for way, (pz, sign) in enumerate(((back, 1), (front, -1))):
                        at = first + 4 * j + 2 * way
                        arrive(px, 1, pz)
                        if (j < 2) == (sign == 1):
                            send(at, px, 1, pz, dz=sign)
                        else:

                            @pl.when(step < 3)
                            def _():
                                send(at, px, 1, pz, dz=sign)

                        send(at + 1, px, 1, pz, flip=True)

            @pl.when(step == 4)
            def _():
                for j, k in enumerate(X_ORDER):
                    px = up(x, k, NX)
                    arrive(px, 1, front)
                    send(first + j, px, 1, front, flip=True)

            z_group(step)
            return carry

        lax.fori_loop(1, 5, ring_step, 0)

        def other_core(i, carry):
            px = up(x, x_rank(i), NX, True)
            for pz in range(NZ):
                arrive(px, 0, pz)
            x_group(x_rank(i))
            return carry

        lax.fori_loop(0, NX, other_core, 0)
        for i in range(15 + 16 * 3 + 4):
            if i in NOT_SENT:
                continue
            remote(xg.at[0, 0, 0], xg.at[0, 0, 0], g_s.at[i], g_r.at[0, 0, 0], dev()).wait_send()

    @pl.when(c == 0)
    def _():
        n = 0
        for m, k in enumerate(Z_ORDER):
            pz = up(z, k, NZ)
            if m:
                arrive(x, 0, pz)
            if m == 0:
                send(n, x, 0, pz, dz=1)
                send(n + 1, x, 0, pz, dz=-1)
                n += 2
            elif k < 3:
                send(n, x, 0, pz, dz=1 if k < 0 else -1)
                n += 1
            send(n, x, 0, pz, dx=1)
            send(n + 1, x, 0, pz, dx=-1)
            send(n + 2, x, 0, pz, flip=True)
            n += 3
        for m, k in enumerate(Z_ORDER):
            pz = up(z, k, NZ)
            for sign in (1, -1):
                px = up(x, -sign, NX)
                arrive(px, 0, pz)
                if (m % 2 == 0) == (sign == 1):
                    send(n, px, 0, pz, dx=sign)
                    n += 1
                send(n, px, 0, pz, flip=True)
                n += 1

        def last_steps(i, carry):
            px = up(x, 2, NX)
            for m in range(2):
                pz = up(z, z_rank(2 * i + m), NZ, True)
                arrive(px, 0, pz)
                send(n + 2 * i + m, px, 0, pz, flip=True)
            x_group(x_rank(i))
            step = i + 1
            for pz in (up(z, lax.rem(step, 4), NZ, True), up(z, NZ - step, NZ, True)):
                for k in range(NX):
                    arrive(k, 1, pz)
            z_group(step)
            return carry

        lax.fori_loop(0, NX, last_steps, 0)

        def sent(i, carry):
            remote(xg.at[0, 0, 0], xg.at[0, 0, 0], g_s.at[i], g_r.at[0, 0, 0], dev()).wait_send()
            return carry

        lax.fori_loop(0, n + 8, sent, 0)

    hx[t] = slots[...].astype(BF16)
    hid_out = [
        remote(hx.at[t], hx.at[t], x_s.at[k - 1], x_r.at[k - 1], dev(dy=k)) for k in (1, 2, 3)
    ]
    for copy in hid_out:
        copy.start()
    edx[t] = ed[:, own_cols]
    for k in (1, 3, 2):
        src = up(t, -k, NY)
        remote(edx.at[src], edx.at[src], ed_s.at[k - 1], ed_r.at[k - 1], dev()).wait_recv()
        remote(hx.at[src], hx.at[src], x_s.at[k - 1], x_r.at[k - 1], dev()).wait_recv()
    result = jnp.zeros((2 * NX * NC * NZ, Q), F32)
    for k in range(NY):
        result = result + dot(hx[k], edx[k]).astype(BF16).astype(F32)
    eo[...] = result.astype(BF16)

    rows = NZ * SEQ

    def part_of(px, pc):
        four = lambda ref: jnp.concatenate([ref[px, pc].reshape(rows, INFO)] * 4, axis=1)
        dense = dot(hd[px, pc].reshape(rows, FF), dd[...])
        routed = dot(st[px, pc].reshape(rows, INFO), eo[...])
        return four(mc) * dense + four(wc) * routed

    pair_out = {}
    for k in (2, 1, 3, 0):
        px = up(x, k, NX)
        s0[k] = part_of(px, 1 - c).astype(BF16)
        pair_out[k] = remote(s0.at[k], r0.at[k], s0_s.at[k], s0_r.at[k], dev(flip=True))
        pair_out[k].start()
        own[k] = part_of(px, c)
    left = slice(0, Q // 2)
    right = slice(Q // 2, Q)
    x_out = []

    def x_send(i, value, dx):
        s1[i] = value.astype(BF16)
        copy = remote(s1.at[i], r1.at[i], s1_s.at[i], s1_r.at[i], dev(dx=dx))
        copy.start()
        x_out.append(copy)

    def x_got(i):
        remote(s1.at[i], r1.at[i], s1_s.at[i], s1_r.at[i], dev()).wait_recv()
        return r1[i].astype(F32)

    for k in (2, 1, 3, 0):
        pair_out[k].wait_recv()
        own[k] = own[k] + r0[k].astype(F32)
        if k == 2:
            x_send(0, own[2, :, left], 1)
            x_send(1, own[2, :, right], -1)
        elif k == 1:
            x_send(2, own[1, :, right], 1)
        elif k == 3:
            x_send(3, own[3, :, left], -1)
    x_send(4, own[1, :, left] + x_got(0), 1)
    x_send(5, own[3, :, right] + x_got(1), -1)
    from_below = [own[0, :, left] + x_got(3), own[0, :, right] + x_got(2)]
    sums = jnp.concatenate([from_below[0] + x_got(4), from_below[1] + x_got(5)], axis=1)
    bsum[...] = sums.reshape(NZ, SEQ, Q)
    s2[...] = sums.astype(BF16).reshape(NZ, SEQ, Q)
    z_out = []
    for k in (4, 3, 5, 2, 6, 1, 7):
        pz = up(z, k, NZ)
        copy = remote(s2.at[pz], r2.at[k - 1], s2_s.at[k - 1], s2_r.at[k - 1], dev(dz=k))
        copy.start()
        z_out.append(copy)
    final = stream_cols.astype(F32) + bsum[z]
    for copy in reversed(z_out):
        copy.wait_recv()
    for k in range(NZ - 1):
        final = final + r2[k].astype(F32)
    out[...] = final

    for copy in heads_out + ed_out + cols_out + hid_out + list(pair_out.values()):
        copy.wait_send()
    for copy in x_out + z_out:
        copy.wait_send()


def layer(*operands):
    vmem = pl.BlockSpec(memory_space=pltpu.VMEM)
    hbm = pl.BlockSpec(memory_space=pltpu.HBM)
    dma = lambda *n: pltpu.SemaphoreType.DMA(n)
    buf = lambda shape, kind=BF16: pltpu.VMEM(shape, kind)
    return pl.pallas_call(
        layer_kernel,
        out_shape=(
            jax.ShapeDtypeStruct((SEQ, Q), F32),
            jax.ShapeDtypeStruct((SEQ, 2 * HEAD_DIM), BF16),
        ),
        in_specs=[hbm] * len(operands),
        out_specs=(vmem, vmem),
        scratch_shapes=[
            buf((SEQ, D)),
            buf((1, SEQ), jnp.int32),
            buf((SEQ, 512, 2 * HEAD_DIM)),
            buf((1, D), F32),
            buf((D, Q + 2 * HEAD_DIM)),
            buf((1, 4), F32),
            buf((1, HEAD_DIM), F32),
            buf((1, D), F32),
            buf((2, SEQ), jnp.int32),
            buf((2, SEQ), F32),
            buf((1, D), F32),
            buf((1, HEAD_DIM), F32),
            buf((SEQ, 8, HEAD_DIM), F32),
            buf((SEQ, HEAD_DIM), F32),
            buf((SEQ, HEAD_DIM), F32),
            buf((SEQ, HEAD_DIM), F32),
            buf((SEQ, 8, HEAD_DIM), F32),
            buf((SEQ, Q)),
            buf((D, Q)),
            buf((D, 4 * FF)),
            buf((INFO, 7 * INFO)),
            buf((FF, D)),
            buf((FF, Q)),
            buf((NY, FF, Q)),
            buf((NY, SEQ, Q)),
            buf((NY, SEQ, Q)),
            buf((NX, NC, NZ, SEQ, WIDE)),
            buf((NX, NC, NZ, SEQ, FF)),
            buf((NX, NC, NZ, SEQ, INFO)),
            buf((NX, NC, NZ, SEQ, INFO), F32),
            buf((NX, NC, NZ, SEQ, INFO), F32),
            buf((NY, 128, FF)),
            buf((128, FF), F32),
            buf((128, Q)),
            buf((NX, NZ * SEQ, Q)),
            buf((NX, NZ * SEQ, Q)),
            buf((NX, NZ * SEQ, Q), F32),
            buf((6, NZ * SEQ, Q // 2)),
            buf((6, NZ * SEQ, Q // 2)),
            buf((NZ, SEQ, Q), F32),
            buf((NZ, SEQ, Q)),
            buf((NZ - 1, SEQ, Q)),
            dma(24),
            dma(3), dma(3), dma(3), dma(3), dma(3), dma(3),
            dma(N_SENDS), dma(NX, NC, NZ),
            dma(3), dma(3), dma(4), dma(4), dma(6), dma(6), dma(7), dma(7),
        ],
        compiler_params=pltpu.CompilerParams(
            collective_id=0, has_side_effects=True, vmem_limit_bytes=60 * 1024 * 1024
        ),
        name="layer",
    )(*operands)


def on_device(
    residual_in, lengths, kv_cache, norm_gain_attn, query_weight, key_weight, value_weight,
    diff_lambda, head_gain, out_weight, norm_gain_ffn, route_ids, route_weights, expert_gate,
    expert_up, expert_down, dense_gate, dense_up, dense_down, dense_mix,
):
    width = residual_in.shape[1]
    half = QK_DIM // 2
    inverse = 10000.0 ** (-np.arange(half, dtype=np.float32) / np.float32(half))
    inverse = np.tile(inverse.astype(np.float32), 4)[None, :]
    final, fresh = layer(
        residual_in,
        lengths.reshape(1, -1),
        kv_cache.reshape(SEQ, 512, 2 * HEAD_DIM),
        norm_gain_attn.reshape(1, width),
        query_weight,
        key_weight,
        value_weight,
        diff_lambda.reshape(1, -1),
        head_gain.reshape(1, -1),
        out_weight,
        norm_gain_ffn.reshape(1, width),
        route_ids.T,
        route_weights.T,
        expert_gate.reshape(width, -1),
        expert_up.reshape(width, -1),
        expert_down.reshape(-1, width),
        dense_gate,
        dense_up,
        dense_down,
        dense_mix.reshape(1, width),
        jnp.asarray(inverse),
    )
    return (final.astype(BF16), fresh.reshape(SEQ, 1, 2 * HEAD_DIM))


def solution(mesh):
    placed = (
        P("ep", None),
        P("ep"),
        P("ep", "tp", None, None),
        P(),
        P(None, "tp"),
        P(None, "tp"),
        P(None, "tp"),
        P("tp"),
        P(),
        P(None, "tp"),
        P(),
        P("ep", None),
        P("ep", None),
        P("ep", None, "tp"),
        P("ep", None, "tp"),
        P("ep", "tp", None),
        P(None, "ep"),
        P(None, "ep"),
        P("ep", None),
        P(),
    )
    return jax.shard_map(
        on_device,
        mesh=mesh,
        in_specs=placed,
        out_specs=(P("ep", "tp"), P("ep", "tp", None)),
        check_vma=False,
    )
```

```python
import jax
import jax.numpy as jnp
import numpy as np
from jax import lax
from jax.experimental import pallas as pl
from jax.experimental.pallas import tpu as pltpu
from jax.sharding import PartitionSpec as P

QK_DIM = 64
HEAD_DIM = 128
EPS = 1e-06
MESH = pl.DeviceIdType.MESH
F32 = jnp.float32
BF16 = jnp.bfloat16
NX, NZ, NY, NC = 4, 8, 4, 2
SEQ = 16
D = 2048
Q = 512
FF = 128
Z_ORDER = (0, -1, 1, -2, 2, -3, 3, 4)
FAR_FIRST = (4, 3, 5, 2, 6, 1, 7)
N_SENDS = 63


def rms_rows(values, gain):
    mean_sq = jnp.mean(values * values, axis=-1, keepdims=True)
    return values * lax.rsqrt(mean_sq + EPS) * gain


def dot(a, b):
    return jnp.dot(a, b, preferred_element_type=F32)


def up(v, n, size, dynamic=False):
    return lax.rem(v + (n if dynamic else n % size), size)


def layer_kernel(
    resid_h, lens_h, kv_h, ga_h, wq_h, wk_h, wv_h, lam_h, hgain_h, wo_h, gf_h, ids_h, rw_h,
    eg_h, eu_h, ed_h, dg_h, du_h, dd_h, mixw_h, inv_h, out, rows_out,
    resid, lens, kv, gain_a, wqkv, lam, hgain, gain, ids_t, rw_t, mix_w, inv,
    qs, fk, fv, lenb, mixed, heads,
    wo, we, wd, ddq, ed, edx, hg, sg, perm, m1s, m1r, m2s, my, hx, eo, n1r, n2s, n2r,
    xd, hd, s0, r0, own, s1, r1, bsum, s2, r2, ys, yr,
    lsem, ed_s, ed_r, h_s, h_r, c_s, c_r, x_s, x_r, y_s, y_r, g_s, g_r, m1_s, m1_q, m2_s, m2_q,
    my_s, my_r, n1_s, n1_q, n2_s, n2_q, s0_s, s0_r, s1_s, s1_r, s2_s, s2_r,
):
    e = lax.axis_index("ep")
    t = lax.axis_index("tp")
    z = lax.div(e, 8)
    x = lax.rem(lax.div(e, 2), 4)
    c = lax.rem(e, 2)

    def dev(dz=0, dx=0, flip=0, dy=0):
        cc = 1 - c if flip else c
        return {
            "ep": (up(z, dz, NZ) * NX + up(x, dx, NX)) * NC + cc,
            "tp": up(t, dy, NY),
        }

    def remote(src, dst, ssem, rsem, to):
        return pltpu.make_async_remote_copy(
            src_ref=src, dst_ref=dst, send_sem=ssem, recv_sem=rsem, device_id=to, device_id_type=MESH
        )

    pairs = [
        (lens_h, lens), (ids_h, ids_t), (rw_h, rw_t), (inv_h, inv), (resid_h, resid), (ga_h, gain_a),
        (wq_h, wqkv.at[:, pl.ds(0, Q)]),
        (wk_h, wqkv.at[:, pl.ds(Q, HEAD_DIM)]),
        (wv_h, wqkv.at[:, pl.ds(Q + HEAD_DIM, HEAD_DIM)]),
        (lam_h, lam), (hgain_h, hgain),
    ]
    pairs += [(kv_h.at[pl.ds(4 * g, 4)], kv.at[pl.ds(4 * g, 4)]) for g in range(4)]
    pairs += [
        (wo_h, wo), (gf_h, gain), (mixw_h, mix_w), (ed_h, ed),
        (eg_h, we.at[:, pl.ds(0, FF)]), (eu_h, we.at[:, pl.ds(FF, FF)]),
        (dg_h, wd.at[:, pl.ds(0, FF)]), (du_h, wd.at[:, pl.ds(FF, FF)]),
    ]
    pairs += [(dd_h.at[:, pl.ds(q * Q, Q)], ddq.at[q]) for q in range(NY)]
    loads = [pltpu.make_async_copy(a, b, lsem.at[i]) for i, (a, b) in enumerate(pairs)]
    for load in loads:
        load.start()
    KV0 = 11
    WO = KV0 + 4

    barrier = pltpu.get_barrier_semaphore()
    peers = (
        [dev(dy=k) for k in (1, 2, 3)]
        + [dev(dx=k) for k in (1, 2, 3)]
        + [dev(dz=k) for k in range(1, 8)]
        + [dev(dx=k, flip=1) for k in (0, 1, 2, 3)]
    )
    for peer in peers:
        pl.semaphore_signal(barrier, inc=1, device_id=peer, device_id_type=MESH)

    for load in loads[:4]:
        load.wait()

    ids = ids_t[...]
    place = ((ids >> 1) & 3) * (NC * NZ * 2) + (ids & 1) * (NZ * 2) + (ids >> 3) * 2
    row16 = lax.broadcasted_iota(jnp.int32, (SEQ, SEQ), 0)
    col16 = lax.broadcasted_iota(jnp.int32, (SEQ, SEQ), 1)
    eye = row16 == col16

    def column(rows, k):
        spread = jnp.broadcast_to(rows[k : k + 1, :], (SEQ, SEQ))
        return jnp.sum(jnp.where(eye, spread, 0.0), axis=1, keepdims=True)

    lane_f = lax.broadcasted_iota(jnp.int32, (SEQ, 128), 1).astype(F32)
    rw = rw_t[...]
    w_cols = [column(rw, k) for k in (0, 1)]
    place_cols = [column(place.astype(F32), k) for k in (0, 1)]
    member = [jnp.where(lane_f == col, 1.0, 0.0) for col in place_cols]
    before = jnp.where(row16 > col16, 1.0, 0.0).astype(BF16)
    earlier = dot(before, (member[0] + member[1]).astype(BF16))
    chosen = []
    for k in (0, 1):
        slot = jnp.sum(member[k] * earlier, axis=1, keepdims=True)
        chosen.append(jnp.where(lane_f == place_cols[k] + slot, 1.0, 0.0).astype(BF16))
    prow = lax.broadcasted_iota(jnp.int32, (128, 128), 0)
    pcol = lax.broadcasted_iota(jnp.int32, (128, 128), 1)
    swapped = ((prow >> 1) & 7) * 16 + (prow >> 4) * 2 + (prow & 1)
    perm[...] = jnp.where(pcol == swapped, 1.0, 0.0).astype(BF16)

    lane1 = lax.broadcasted_iota(jnp.int32, (SEQ, HEAD_DIM), 1)
    length = column(lens[...].astype(F32), 0)
    lenb[...] = jnp.broadcast_to(length, (SEQ, HEAD_DIM))
    angle = length * inv[...]
    cosine = jnp.cos(angle)
    low = lax.rem(lane1, QK_DIM) < QK_DIM // 2
    sine = jnp.where(low, -jnp.sin(angle), jnp.sin(angle))

    def turned(v):
        ahead = pltpu.roll(v, HEAD_DIM - QK_DIM // 2, 1)
        behind = pltpu.roll(v, QK_DIM // 2, 1)
        return (v * cosine + jnp.where(low, ahead, behind) * sine).astype(BF16)

    for load in loads[4:6]:
        load.wait()
    normed = rms_rows(resid[...].astype(F32), gain_a[...]).astype(BF16)
    for load in loads[6:KV0]:
        load.wait()
    proj = dot(normed, wqkv[...])
    key_new = turned(proj[:, Q : Q + HEAD_DIM])
    val_new = proj[:, Q + HEAD_DIM :].astype(BF16)
    rows_out[:, 0:HEAD_DIM] = key_new
    rows_out[:, HEAD_DIM:] = val_new
    fk[...] = key_new.astype(F32)
    fv[...] = val_new.astype(F32)
    first = lane1 < QK_DIM
    turned_q = [turned(proj[:, j * HEAD_DIM : (j + 1) * HEAD_DIM]) for j in range(4)]
    zero = jnp.zeros((SEQ, HEAD_DIM), BF16)
    stack = jnp.concatenate(
        [jnp.where(first, q, zero) for q in turned_q] + [jnp.where(first, zero, q) for q in turned_q],
        axis=0,
    )
    to_seq = lax.rem(prow, 8) * SEQ + lax.div(prow, 8) == pcol
    to_head = lax.rem(prow, SEQ) * 8 + lax.div(prow, SEQ) == pcol
    qs[...] = dot(jnp.where(to_seq, 1.0, 0.0).astype(BF16), stack).reshape(SEQ, 8, HEAD_DIM)

    srow = lax.broadcasted_iota(jnp.int32, (8, 4), 0)
    scol = lax.broadcasted_iota(jnp.int32, (8, 4), 1)
    lam_col = jnp.sum(
        jnp.where(srow - 4 == scol, jnp.broadcast_to(lam[...], (8, 4)), 0.0), axis=1, keepdims=True
    )
    sign = jnp.where(lax.broadcasted_iota(jnp.int32, (8, 1), 0) < 4, 1.0, -lam_col)
    sign4 = jnp.concatenate([sign] * 4, axis=0)
    position = lax.broadcasted_iota(jnp.int32, (32, 512), 1).astype(F32)
    scale = QK_DIM ** (-0.5)
    contract_last = (((1,), (1,)), ((), ()))
    for load in loads[KV0:WO]:
        load.wait()
    for g in range(4):
        seqs = range(4 * g, 4 * g + 4)
        q4 = [qs[b] for b in seqs]
        scores = jnp.concatenate(
            [
                lax.dot_general(
                    q.astype(BF16), kv[b, :, 0:HEAD_DIM], contract_last, preferred_element_type=F32
                )
                for q, b in zip(q4, seqs)
            ],
            axis=0,
        )
        latest = scale * jnp.concatenate(
            [jnp.sum(q * fk[b : b + 1, :], axis=1, keepdims=True) for q, b in zip(q4, seqs)], axis=0
        )
        count = jnp.concatenate([jnp.broadcast_to(lenb[b : b + 1, 0:1], (8, 1)) for b in seqs], axis=0)
        masked = jnp.where(position < count, scores * scale, -1e30)
        top = jnp.maximum(jnp.max(masked, axis=1, keepdims=True), latest)
        raised = jnp.exp(masked - top)
        raised_new = jnp.exp(latest - top)
        weight = sign4 / (jnp.sum(raised, axis=1, keepdims=True) + raised_new)
        both = raised * weight
        mapped = (both + pltpu.roll(both, 28, 0)).astype(BF16)
        new = jnp.broadcast_to(raised_new * weight, (32, HEAD_DIM))
        mapped_new = (new + pltpu.roll(new, 28, 0)).astype(BF16).astype(F32)
        for i, b in enumerate(seqs):
            at = slice(8 * i, 8 * i + 8)
            mixed[b] = dot(mapped[at, :], kv[b, :, HEAD_DIM:]) + mapped_new[at, :] * fv[b : b + 1, :]
    normed_heads = rms_rows(mixed[...].reshape(128, HEAD_DIM), hgain[...]).astype(BF16)
    by_head = dot(jnp.where(to_head, 1.0, 0.0).astype(BF16), normed_heads).astype(BF16)
    for j in range(4):
        heads[:, j * HEAD_DIM : (j + 1) * HEAD_DIM] = by_head[j * SEQ : (j + 1) * SEQ, :]

    pl.semaphore_wait(barrier, 17)

    heads_out = [
        remote(heads, hg.at[t], h_s.at[k - 1], h_r.at[k - 1], dev(dy=k)) for k in (1, 2, 3)
    ]
    for copy in heads_out:
        copy.start()
    own_cols = pl.ds(pl.multiple_of(t * Q, Q), Q)
    for load in loads[WO:WO + 4]:
        load.wait()

    def wo_rows(src):
        return wo[pl.ds(pl.multiple_of(src * Q, Q), Q), :]

    total = resid[:, own_cols].astype(F32) + dot(heads[...], wo_rows(t))
    for k in (1, 3, 2):
        src = up(t, -k, NY)
        remote(heads, hg.at[src], h_s.at[k - 1], h_r.at[k - 1], dev()).wait_recv()
        total = total + dot(hg[src], wo_rows(src))
    stream_cols = total.astype(BF16)
    sg[t] = stream_cols
    done = heads_out
    started = []

    def begin(src, dst, ssem, rsem, **to):
        copy = remote(src, dst, ssem, rsem, dev(**to))
        copy.start()
        started.append(copy)

    def landed(ref, rsem):
        remote(ref, ref, rsem, rsem, dev()).wait_recv()

    for k in (2, 1, 3):
        begin(sg.at[t], sg.at[t], c_s.at[k - 1], c_r.at[k - 1], dy=k)

    xc = x * NC + c
    outgoing = lax.dot_general(
        (chosen[0] + chosen[1]), stream_cols, (((0,), (0,)), ((), ())), preferred_element_type=F32
    )
    m1s[...] = outgoing.astype(BF16).reshape(NX * NC, SEQ, Q)
    plane = [(dx, flip) for dx in (2, 1, 3) for flip in (0, 1)] + [(0, 1)]

    def other(dx, flip):
        return up(x, dx, NX) * NC + (1 - c if flip else c)

    for i, (dx, flip) in enumerate(plane):
        begin(m1s.at[other(dx, flip)], m1r.at[xc], m1_s.at[i], m1_q.at[i], dx=dx, flip=flip)
    m1r[xc] = m1s[xc]
    for k in (2, 1, 3):
        cols = pl.ds(pl.multiple_of(up(t, k, NY) * Q, Q), Q)
        begin(ed.at[:, cols], edx.at[t], ed_s.at[k - 1], ed_r.at[k - 1], dy=k)

    for k in (1, 3, 2):
        src = up(t, -k, NY)
        landed(sg.at[src], c_r.at[k - 1])
    stream = jnp.concatenate([sg[k] for k in range(NY)], axis=1).astype(F32)
    ffn_in = rms_rows(stream, gain[...]).astype(BF16)
    mine = 4 * t + (row16 & 3) == col16
    block = jnp.zeros((SEQ, Q), F32)
    for q in range(NY):
        pick = jnp.where(mine & ((row16 >> 2) == q), 1.0, 0.0).astype(BF16)
        block = block + dot(pick, ffn_in[:, q * Q : (q + 1) * Q])
    xd[x, c, z] = block.astype(BF16)
    sends = [0]

    def give(px, pz, **to):
        i = sends[0]
        sends[0] += 1
        begin(xd.at[px, c, pz], xd.at[px, c, pz], g_s.at[i], g_r.at[px, c, pz], **to)

    def arrive(px, pc, pz):
        landed(xd.at[px, pc, pz], g_r.at[px, pc, pz])

    for k in FAR_FIRST:
        give(x, z, dz=k)
    give(x, z, dx=1)
    give(x, z, dx=-1)
    give(x, z, flip=1)
    mix = jax.nn.sigmoid(jnp.sum(ffn_in.astype(F32) * mix_w[...], axis=-1, keepdims=True))
    mix_row = jnp.sum(jnp.where(eye, jnp.broadcast_to(mix, (SEQ, SEQ)), 0.0), axis=0, keepdims=True)
    mix_mine = jnp.sum(jnp.where(mine, jnp.broadcast_to(mix_row, (SEQ, SEQ)), 0.0), axis=1, keepdims=True)

    def regroup(ref):
        return dot(perm[...], ref[...].reshape(128, Q)).astype(BF16).reshape(8, SEQ, Q)

    for i, (dx, flip) in enumerate(plane):
        landed(m1r.at[other(-dx, flip)], m1_q.at[i])
    m2s[...] = regroup(m1r)
    for k in FAR_FIRST:
        begin(m2s.at[up(z, k, NZ)], my.at[t, z], m2_s.at[k - 1], m2_q.at[k - 1], dz=k)
    my[t, z] = m2s[z]

    for k in Z_ORDER[1:]:
        pz = up(z, k, NZ)
        arrive(x, c, pz)
        give(x, pz, dx=1)
        give(x, pz, dx=-1)
        give(x, pz, flip=1)

    count = [0]

    def pass_on(pt, pz, dy):
        i = count[0]
        count[0] += 1
        begin(my.at[pt, pz], my.at[pt, pz], my_s.at[i], my_r.at[pt, pz], dy=dy)

    for k in Z_ORDER:
        pz = up(z, k, NZ)
        if k:
            landed(my.at[t, pz], m2_q.at[(-k) % NZ - 1])
        pass_on(t, pz, 1)
        pass_on(t, pz, -1)

    for m, k in enumerate(Z_ORDER):
        pz = up(z, k, NZ)
        for way in (1, -1):
            px = up(x, -way, NX)
            arrive(px, c, pz)
            if (m % 2 == 0) == (way == 1):
                give(px, pz, dx=way)
            give(px, pz, flip=1)
    for m, k in enumerate(Z_ORDER):
        pz = up(z, k, NZ)
        for way in (1, -1):
            pt = up(t, -way, NY)
            landed(my.at[pt, pz], my_r.at[pt, pz])
            if (m % 2 == 0) == (way == 1):
                pass_on(pt, pz, way)
    for k in Z_ORDER:
        pz = up(z, k, NZ)
        px = up(x, 2, NX)
        arrive(px, c, pz)
        give(px, pz, flip=1)

    for load in loads[WO + 4 :]:
        load.wait()
    drow = lax.broadcasted_iota(jnp.int32, (256, 1), 0)
    quarter = (drow >> 2) & 3
    low_rows = (lax.broadcasted_iota(jnp.int32, (128, 1), 0) & 7) < 4

    def by_quarter(value):
        which = quarter[0 : value.shape[0]]
        return jnp.concatenate([jnp.where(which == q, value, jnp.zeros_like(value)) for q in range(NY)], axis=1)

    def dense_rows(px):
        both = dot(by_quarter(xd[px].reshape(256, Q)), wd[...]).reshape(16, 2, 8, 2 * FF)
        half = (both[:, 0] + both[:, 1]).reshape(128, 2 * FF)
        full = half + jnp.where(low_rows, pltpu.roll(half, 124, 0), pltpu.roll(half, 4, 0))
        hidden = (jax.nn.silu(full[:, 0:FF]) * full[:, FF:]).reshape(16, 8, FF)
        hd[px] = jnp.concatenate([hidden, hidden], axis=1).astype(BF16).reshape(NC, NZ, SEQ, FF)

    def part_of(px, pc):
        return dot(by_quarter(hd[px, pc].reshape(128, FF)), ddq[...].reshape(NY * FF, Q))

    for k in (2, 1, 3, 0):
        px = up(x, k, NX)
        for pz in range(NZ):
            arrive(px, 1 - c, pz)
        dense_rows(px)
        s0[k] = part_of(px, 1 - c).astype(BF16)
        begin(s0.at[k], r0.at[k], s0_s.at[k], s0_r.at[k], flip=1)
        own[k] = part_of(px, c)

    for k in Z_ORDER:
        pz = up(z, k, NZ)
        pt = up(t, 2, NY)
        landed(my.at[pt, pz], my_r.at[pt, pz])
    rows_in = jnp.concatenate([my[k].reshape(128, Q) for k in range(NY)], axis=1).astype(F32)
    both = dot(rms_rows(rows_in, gain[...]).astype(BF16), we[...])
    hx[t] = (jax.nn.silu(both[:, 0:FF]) * both[:, FF:]).astype(BF16)
    for k in (2, 1, 3):
        begin(hx.at[t], hx.at[t], x_s.at[k - 1], x_r.at[k - 1], dy=k)

    left = slice(0, Q // 2)
    right = slice(Q // 2, Q)

    def x_send(i, value, dx):
        s1[i] = value.astype(BF16)
        begin(s1.at[i], r1.at[i], s1_s.at[i], s1_r.at[i], dx=dx)

    def x_got(i):
        landed(r1.at[i], s1_r.at[i])
        return r1[i].astype(F32)

    for k in (2, 1, 3, 0):
        landed(r0.at[k], s0_r.at[k])
        own[k] = own[k] + r0[k].astype(F32)
        if k == 2:
            x_send(0, own[2, :, left], 1)
            x_send(1, own[2, :, right], -1)
        elif k == 1:
            x_send(2, own[1, :, right], 1)
        elif k == 3:
            x_send(3, own[3, :, left], -1)
    x_send(4, own[1, :, left] + x_got(0), 1)
    x_send(5, own[3, :, right] + x_got(1), -1)

    own_q = pl.ds(pl.multiple_of(t * Q, Q), Q)
    edx[t] = ed[:, own_q]
    for k in (1, 3, 2):
        src = up(t, -k, NY)
        landed(edx.at[src], ed_r.at[k - 1])
        landed(hx.at[src], x_r.at[k - 1])
    result = jnp.zeros((128, Q), F32)
    for k in range(NY):
        result = result + dot(hx[k], edx[k]).astype(BF16).astype(F32)
    eo[...] = result.astype(BF16).reshape(NZ, SEQ, Q)
    for k in FAR_FIRST:
        begin(eo.at[up(z, k, NZ)], n1r.at[z], n1_s.at[k - 1], n1_q.at[k - 1], dz=k)
    n1r[z] = eo[z]

    from_sides = [own[0, :, left] + x_got(3), own[0, :, right] + x_got(2)]
    sums = jnp.concatenate([from_sides[0] + x_got(4), from_sides[1] + x_got(5)], axis=1)
    bsum[...] = sums.reshape(NZ, SEQ, Q)
    s2[...] = sums.astype(BF16).reshape(NZ, SEQ, Q)
    for k in FAR_FIRST:
        begin(s2.at[up(z, k, NZ)], r2.at[k - 1], s2_s.at[k - 1], s2_r.at[k - 1], dz=k)

    for k in reversed(FAR_FIRST):
        landed(n1r.at[up(z, -k, NZ)], n1_q.at[k - 1])
    n2s[...] = regroup(n1r)
    for i, (dx, flip) in enumerate(plane):
        begin(n2s.at[other(dx, flip)], n2r.at[xc], n2_s.at[i], n2_q.at[i], dx=dx, flip=flip)
    n2r[xc] = n2s[xc]

    for k in reversed(FAR_FIRST):
        landed(r2.at[k - 1], s2_r.at[k - 1])
    dense = bsum[z]
    for k in range(NZ - 1):
        dense = dense + r2[k].astype(F32)
    dense = dense * mix_mine
    for q in range(NY):
        four = dense[4 * q : 4 * q + 4, :]
        ys[q] = jnp.concatenate([four, four], axis=0)
    yr[t] = ys[t]
    for k in (2, 1, 3):
        begin(ys.at[up(t, k, NY)], yr.at[t], y_s.at[k - 1], y_r.at[k - 1], dy=k)

    for i, (dx, flip) in enumerate(plane):
        landed(n2r.at[other(-dx, flip)], n2_q.at[i])
    back = n2r[...].reshape(128, Q)
    final = stream_cols.astype(F32)
    moe = w_cols[0] * dot(chosen[0], back) + w_cols[1] * dot(chosen[1], back)
    for k in (1, 3, 2):
        src = up(t, -k, NY)
        landed(yr.at[src], y_r.at[k - 1])
    dense_cols = jnp.concatenate([yr[k, 0:4, :] for k in range(NY)], axis=0)
    out[...] = final + moe + dense_cols

    for copy in done + started:
        copy.wait_send()


def layer(*operands):
    vmem = pl.BlockSpec(memory_space=pltpu.VMEM)
    hbm = pl.BlockSpec(memory_space=pltpu.HBM)
    dma = lambda *n: pltpu.SemaphoreType.DMA(n)
    buf = lambda shape, kind=BF16: pltpu.VMEM(shape, kind)
    return pl.pallas_call(
        layer_kernel,
        out_shape=(
            jax.ShapeDtypeStruct((SEQ, Q), F32),
            jax.ShapeDtypeStruct((SEQ, 2 * HEAD_DIM), BF16),
        ),
        in_specs=[hbm] * len(operands),
        out_specs=(vmem, vmem),
        scratch_shapes=[
            buf((SEQ, D)),
            buf((1, SEQ), jnp.int32),
            buf((SEQ, 512, 2 * HEAD_DIM)),
            buf((1, D), F32),
            buf((D, Q + 2 * HEAD_DIM)),
            buf((1, 4), F32),
            buf((1, HEAD_DIM), F32),
            buf((1, D), F32),
            buf((2, SEQ), jnp.int32),
            buf((2, SEQ), F32),
            buf((1, D), F32),
            buf((1, HEAD_DIM), F32),
            buf((SEQ, 8, HEAD_DIM), F32),
            buf((SEQ, HEAD_DIM), F32),
            buf((SEQ, HEAD_DIM), F32),
            buf((SEQ, HEAD_DIM), F32),
            buf((SEQ, 8, HEAD_DIM), F32),
            buf((SEQ, Q)),
            buf((D, Q)),
            buf((D, 2 * FF)),
            buf((D, 2 * FF)),
            buf((NY, FF, Q)),
            buf((FF, D)),
            buf((NY, FF, Q)),
            buf((NY, SEQ, Q)),
            buf((NY, SEQ, Q)),
            buf((128, 128)),
            buf((8, SEQ, Q)),
            buf((8, SEQ, Q)),
            buf((8, SEQ, Q)),
            buf((NY, NZ, SEQ, Q)),
            buf((NY, 128, FF)),
            buf((8, SEQ, Q)),
            buf((8, SEQ, Q)),
            buf((8, SEQ, Q)),
            buf((8, SEQ, Q)),
            buf((NX, NC, NZ, SEQ, Q)),
            buf((NX, NC, NZ, SEQ, FF)),
            buf((NX, NZ * SEQ, Q)),
            buf((NX, NZ * SEQ, Q)),
            buf((NX, NZ * SEQ, Q), F32),
            buf((6, NZ * SEQ, Q // 2)),
            buf((6, NZ * SEQ, Q // 2)),
            buf((NZ, SEQ, Q), F32),
            buf((NZ, SEQ, Q)),
            buf((NZ - 1, SEQ, Q)),
            buf((NY, 8, Q), F32),
            buf((NY, 8, Q), F32),
            dma(27),
            dma(3), dma(3), dma(3), dma(3), dma(3), dma(3), dma(3), dma(3), dma(3), dma(3),
            dma(N_SENDS), dma(NX, NC, NZ),
            dma(7), dma(7), dma(7), dma(7),
            dma(24), dma(NY, NZ),
            dma(7), dma(7), dma(7), dma(7),
            dma(4), dma(4), dma(6), dma(6), dma(7), dma(7),
        ],
        compiler_params=pltpu.CompilerParams(
            collective_id=0, has_side_effects=True, vmem_limit_bytes=60 * 1024 * 1024
        ),
        name="layer",
    )(*operands)


def on_device(
    residual_in, lengths, kv_cache, norm_gain_attn, query_weight, key_weight, value_weight,
    diff_lambda, head_gain, out_weight, norm_gain_ffn, route_ids, route_weights, expert_gate,
    expert_up, expert_down, dense_gate, dense_up, dense_down, dense_mix,
):
    width = residual_in.shape[1]
    half = QK_DIM // 2
    inverse = 10000.0 ** (-np.arange(half, dtype=np.float32) / np.float32(half))
    inverse = np.tile(inverse.astype(np.float32), 4)[None, :]
    final, fresh = layer(
        residual_in,
        lengths.reshape(1, -1),
        kv_cache.reshape(SEQ, 512, 2 * HEAD_DIM),
        norm_gain_attn.reshape(1, width),
        query_weight,
        key_weight,
        value_weight,
        diff_lambda.reshape(1, -1),
        head_gain.reshape(1, -1),
        out_weight,
        norm_gain_ffn.reshape(1, width),
        route_ids.T,
        route_weights.T,
        expert_gate.reshape(width, -1),
        expert_up.reshape(width, -1),
        expert_down.reshape(-1, width),
        dense_gate,
        dense_up,
        dense_down,
        dense_mix.reshape(1, width),
        jnp.asarray(inverse),
    )
    return (final.astype(BF16), fresh.reshape(SEQ, 1, 2 * HEAD_DIM))


def solution(mesh):
    placed = (
        P("ep", None),
        P("ep"),
        P("ep", "tp", None, None),
        P(),
        P(None, "tp"),
        P(None, "tp"),
        P(None, "tp"),
        P("tp"),
        P(),
        P(None, "tp"),
        P(),
        P("ep", None),
        P("ep", None),
        P("ep", None, "tp"),
        P("ep", None, "tp"),
        P("ep", "tp", None),
        P(None, "ep"),
        P(None, "ep"),
        P("ep", None),
        P(),
    )
    return jax.shard_map(
        on_device,
        mesh=mesh,
        in_specs=placed,
        out_specs=(P("ep", "tp"), P("ep", "tp", None)),
        check_vma=False,
    )
```

```python
import jax
import jax.numpy as jnp
import numpy as np
from jax import lax
from jax.experimental import pallas as pl
from jax.experimental.pallas import tpu as pltpu
from jax.sharding import PartitionSpec as P

QK_DIM = 64
HEAD_DIM = 128
EPS = 1e-06
MESH = pl.DeviceIdType.MESH
F32 = jnp.float32
BF16 = jnp.bfloat16
NX, NZ, NY, NC = 4, 8, 4, 2
SEQ = 16
D = 2048
Q = 512
FF = 128
Z_ORDER = (0, -1, 1, -2, 2, -3, 3, 4)
FAR_FIRST = (4, 3, 5, 2, 6, 1, 7)
N_SENDS = 63


def rms_rows(values, gain):
    mean_sq = jnp.mean(values * values, axis=-1, keepdims=True)
    return values * lax.rsqrt(mean_sq + EPS) * gain


def dot(a, b):
    return jnp.dot(a, b, preferred_element_type=F32)


def up(v, n, size, dynamic=False):
    return lax.rem(v + (n if dynamic else n % size), size)


def layer_kernel(
    resid_h, lens_h, kv_h, ga_h, wq_h, wk_h, wv_h, lam_h, hgain_h, wo_h, gf_h, ids_h, rw_h,
    eg_h, eu_h, ed_h, dg_h, du_h, dd_h, mixw_h, inv_h, out, rows_out,
    resid, lens, kv, gain_a, wqkv, lam, hgain, gain, ids_t, rw_t, mix_w, inv,
    qs, fk, fv, lenb, mixed, heads,
    wo, we, wd, ddq, ed, edx, hg, sg, perm, m1s, m1r, m2s, my, hx, eo, n1r, n2s, n2r,
    xd, s0, r0, own, s1, r1, bsum, s2, r2, ys, yr,
    lsem, ed_s, ed_r, h_s, h_r, c_s, c_r, x_s, x_r, y_s, y_r, g_s, g_r, m1_s, m1_q, m2_s, m2_q,
    my_s, my_r, n1_s, n1_q, n2_s, n2_q, s0_s, s0_r, s1_s, s1_r, s2_s, s2_r,
):
    e = lax.axis_index("ep")
    t = lax.axis_index("tp")
    z = lax.div(e, 8)
    x = lax.rem(lax.div(e, 2), 4)
    c = lax.rem(e, 2)

    def dev(dz=0, dx=0, flip=0, dy=0):
        cc = 1 - c if flip else c
        return {
            "ep": (up(z, dz, NZ) * NX + up(x, dx, NX)) * NC + cc,
            "tp": up(t, dy, NY),
        }

    def remote(src, dst, ssem, rsem, to):
        return pltpu.make_async_remote_copy(
            src_ref=src, dst_ref=dst, send_sem=ssem, recv_sem=rsem, device_id=to, device_id_type=MESH
        )

    pairs = {
        "wq": (wq_h, wqkv.at[:, pl.ds(0, Q)]),
        "wk": (wk_h, wqkv.at[:, pl.ds(Q, HEAD_DIM)]),
        "wv": (wv_h, wqkv.at[:, pl.ds(Q + HEAD_DIM, HEAD_DIM)]),
        "resid": (resid_h, resid),
        "gain_a": (ga_h, gain_a),
        "lens": (lens_h, lens),
        "inv": (inv_h, inv),
        "ids": (ids_h, ids_t),
        "rw": (rw_h, rw_t),
        "lam": (lam_h, lam),
        "hgain": (hgain_h, hgain),
    }
    for g in range(4):
        pairs[f"kv{g}"] = (kv_h.at[pl.ds(4 * g, 4)], kv.at[pl.ds(4 * g, 4)])
    pairs |= {
        "wo": (wo_h, wo),
        "gain": (gf_h, gain),
        "mix": (mixw_h, mix_w),
        "ed": (ed_h, ed),
        "dg": (dg_h, wd.at[:, pl.ds(0, FF)]),
        "du": (du_h, wd.at[:, pl.ds(FF, FF)]),
        "eg": (eg_h, we.at[:, pl.ds(0, FF)]),
        "eu": (eu_h, we.at[:, pl.ds(FF, FF)]),
    }
    for q in range(NY):
        pairs[f"dd{q}"] = (dd_h.at[:, pl.ds(q * Q, Q)], ddq.at[q])
    loads = {
        name: pltpu.make_async_copy(a, b, lsem.at[i]) for i, (name, (a, b)) in enumerate(pairs.items())
    }
    for load in loads.values():
        load.start()

    def loaded(*names):
        for name in names:
            loads[name].wait()

    barrier = pltpu.get_barrier_semaphore()
    peers = (
        [dev(dy=k) for k in (1, 2, 3)]
        + [dev(dx=k) for k in (1, 2, 3)]
        + [dev(dz=k) for k in range(1, 8)]
        + [dev(dx=k, flip=1) for k in (0, 1, 2, 3)]
    )
    for peer in peers:
        pl.semaphore_signal(barrier, inc=1, device_id=peer, device_id_type=MESH)

    loaded("lens", "inv", "ids", "rw")

    ids = ids_t[...]
    place = ((ids >> 1) & 3) * (NC * NZ * 2) + (ids & 1) * (NZ * 2) + (ids >> 3) * 2
    row16 = lax.broadcasted_iota(jnp.int32, (SEQ, SEQ), 0)
    col16 = lax.broadcasted_iota(jnp.int32, (SEQ, SEQ), 1)
    eye = row16 == col16

    def column(rows, k):
        spread = jnp.broadcast_to(rows[k : k + 1, :], (SEQ, SEQ))
        return jnp.sum(jnp.where(eye, spread, 0.0), axis=1, keepdims=True)

    lane_f = lax.broadcasted_iota(jnp.int32, (SEQ, 128), 1).astype(F32)
    rw = rw_t[...]
    w_cols = [column(rw, k) for k in (0, 1)]
    place_cols = [column(place.astype(F32), k) for k in (0, 1)]
    member = [jnp.where(lane_f == col, 1.0, 0.0) for col in place_cols]
    before = jnp.where(row16 > col16, 1.0, 0.0).astype(BF16)
    earlier = dot(before, (member[0] + member[1]).astype(BF16))
    chosen = []
    for k in (0, 1):
        slot = jnp.sum(member[k] * earlier, axis=1, keepdims=True)
        chosen.append(jnp.where(lane_f == place_cols[k] + slot, 1.0, 0.0).astype(BF16))
    prow = lax.broadcasted_iota(jnp.int32, (128, 128), 0)
    pcol = lax.broadcasted_iota(jnp.int32, (128, 128), 1)
    swapped = ((prow >> 1) & 7) * 16 + (prow >> 4) * 2 + (prow & 1)
    perm[...] = jnp.where(pcol == swapped, 1.0, 0.0).astype(BF16)

    lane1 = lax.broadcasted_iota(jnp.int32, (SEQ, HEAD_DIM), 1)
    length = column(lens[...].astype(F32), 0)
    lenb[...] = jnp.broadcast_to(length, (SEQ, HEAD_DIM))
    angle = length * inv[...]
    cosine = jnp.cos(angle)
    low = lax.rem(lane1, QK_DIM) < QK_DIM // 2
    sine = jnp.where(low, -jnp.sin(angle), jnp.sin(angle))

    def turned(v):
        ahead = pltpu.roll(v, HEAD_DIM - QK_DIM // 2, 1)
        behind = pltpu.roll(v, QK_DIM // 2, 1)
        return (v * cosine + jnp.where(low, ahead, behind) * sine).astype(BF16)

    loaded("resid", "gain_a")
    normed = rms_rows(resid[...].astype(F32), gain_a[...]).astype(BF16)
    loaded("wq", "wk", "wv", "lam", "hgain")
    proj = dot(normed, wqkv[...])
    key_new = turned(proj[:, Q : Q + HEAD_DIM])
    val_new = proj[:, Q + HEAD_DIM :].astype(BF16)
    rows_out[:, 0:HEAD_DIM] = key_new
    rows_out[:, HEAD_DIM:] = val_new
    fk[...] = key_new.astype(F32)
    fv[...] = val_new.astype(F32)
    first = lane1 < QK_DIM
    turned_q = [turned(proj[:, j * HEAD_DIM : (j + 1) * HEAD_DIM]) for j in range(4)]
    zero = jnp.zeros((SEQ, HEAD_DIM), BF16)
    stack = jnp.concatenate(
        [jnp.where(first, q, zero) for q in turned_q] + [jnp.where(first, zero, q) for q in turned_q],
        axis=0,
    )
    to_seq = lax.rem(prow, 8) * SEQ + lax.div(prow, 8) == pcol
    to_head = lax.rem(prow, SEQ) * 8 + lax.div(prow, SEQ) == pcol
    qs[...] = dot(jnp.where(to_seq, 1.0, 0.0).astype(BF16), stack).reshape(SEQ, 8, HEAD_DIM)

    srow = lax.broadcasted_iota(jnp.int32, (8, 4), 0)
    scol = lax.broadcasted_iota(jnp.int32, (8, 4), 1)
    lam_col = jnp.sum(
        jnp.where(srow - 4 == scol, jnp.broadcast_to(lam[...], (8, 4)), 0.0), axis=1, keepdims=True
    )
    sign = jnp.where(lax.broadcasted_iota(jnp.int32, (8, 1), 0) < 4, 1.0, -lam_col)
    sign4 = jnp.concatenate([sign] * 4, axis=0)
    position = lax.broadcasted_iota(jnp.int32, (32, 512), 1).astype(F32)
    scale = QK_DIM ** (-0.5)
    contract_last = (((1,), (1,)), ((), ()))
    loaded("kv0", "kv1", "kv2", "kv3")
    for g in range(4):
        seqs = range(4 * g, 4 * g + 4)
        q4 = [qs[b] for b in seqs]
        scores = jnp.concatenate(
            [
                lax.dot_general(
                    q.astype(BF16), kv[b, :, 0:HEAD_DIM], contract_last, preferred_element_type=F32
                )
                for q, b in zip(q4, seqs)
            ],
            axis=0,
        )
        latest = scale * jnp.concatenate(
            [jnp.sum(q * fk[b : b + 1, :], axis=1, keepdims=True) for q, b in zip(q4, seqs)], axis=0
        )
        count = jnp.concatenate([jnp.broadcast_to(lenb[b : b + 1, 0:1], (8, 1)) for b in seqs], axis=0)
        masked = jnp.where(position < count, scores * scale, -1e30)
        top = jnp.maximum(jnp.max(masked, axis=1, keepdims=True), latest)
        raised = jnp.exp(masked - top)
        raised_new = jnp.exp(latest - top)
        weight = sign4 / (jnp.sum(raised, axis=1, keepdims=True) + raised_new)
        both = raised * weight
        mapped = (both + pltpu.roll(both, 28, 0)).astype(BF16)
        new = jnp.broadcast_to(raised_new * weight, (32, HEAD_DIM))
        mapped_new = (new + pltpu.roll(new, 28, 0)).astype(BF16).astype(F32)
        for i, b in enumerate(seqs):
            at = slice(8 * i, 8 * i + 8)
            mixed[b] = dot(mapped[at, :], kv[b, :, HEAD_DIM:]) + mapped_new[at, :] * fv[b : b + 1, :]
    normed_heads = rms_rows(mixed[...].reshape(128, HEAD_DIM), hgain[...]).astype(BF16)
    by_head = dot(jnp.where(to_head, 1.0, 0.0).astype(BF16), normed_heads).astype(BF16)
    for j in range(4):
        heads[:, j * HEAD_DIM : (j + 1) * HEAD_DIM] = by_head[j * SEQ : (j + 1) * SEQ, :]

    pl.semaphore_wait(barrier, 17)

    heads_out = [
        remote(heads, hg.at[t], h_s.at[k - 1], h_r.at[k - 1], dev(dy=k)) for k in (1, 2, 3)
    ]
    for copy in heads_out:
        copy.start()
    own_cols = pl.ds(pl.multiple_of(t * Q, Q), Q)
    loaded("wo", "gain", "mix", "ed")

    def wo_rows(src):
        return wo[pl.ds(pl.multiple_of(src * Q, Q), Q), :]

    total = resid[:, own_cols].astype(F32) + dot(heads[...], wo_rows(t))
    for k in (1, 3, 2):
        src = up(t, -k, NY)
        remote(heads, hg.at[src], h_s.at[k - 1], h_r.at[k - 1], dev()).wait_recv()
        total = total + dot(hg[src], wo_rows(src))
    stream_cols = total.astype(BF16)
    sg[t] = stream_cols
    done = heads_out
    started = []

    def begin(src, dst, ssem, rsem, **to):
        copy = remote(src, dst, ssem, rsem, dev(**to))
        copy.start()
        started.append(copy)

    def landed(ref, rsem):
        remote(ref, ref, rsem, rsem, dev()).wait_recv()

    for k in (2, 1, 3):
        begin(sg.at[t], sg.at[t], c_s.at[k - 1], c_r.at[k - 1], dy=k)

    xc = x * NC + c
    outgoing = lax.dot_general(
        (chosen[0] + chosen[1]), stream_cols, (((0,), (0,)), ((), ())), preferred_element_type=F32
    )
    m1s[...] = outgoing.astype(BF16).reshape(NX * NC, SEQ, Q)
    plane = [(dx, flip) for dx in (2, 1, 3) for flip in (0, 1)] + [(0, 1)]

    def other(dx, flip):
        return up(x, dx, NX) * NC + (1 - c if flip else c)

    for i, (dx, flip) in enumerate(plane):
        begin(m1s.at[other(dx, flip)], m1r.at[xc], m1_s.at[i], m1_q.at[i], dx=dx, flip=flip)
    m1r[xc] = m1s[xc]
    for k in (2, 1, 3):
        cols = pl.ds(pl.multiple_of(up(t, k, NY) * Q, Q), Q)
        begin(ed.at[:, cols], edx.at[t], ed_s.at[k - 1], ed_r.at[k - 1], dy=k)

    for k in (1, 3, 2):
        src = up(t, -k, NY)
        landed(sg.at[src], c_r.at[k - 1])
    stream = jnp.concatenate([sg[k] for k in range(NY)], axis=1).astype(F32)
    ffn_in = rms_rows(stream, gain[...]).astype(BF16)
    mine = 4 * t + (row16 & 3) == col16
    block = jnp.zeros((SEQ, Q), F32)
    for q in range(NY):
        pick = jnp.where(mine & ((row16 >> 2) == q), 1.0, 0.0).astype(BF16)
        block = block + dot(pick, ffn_in[:, q * Q : (q + 1) * Q])
    xd[x, c, z] = block.astype(BF16)
    sends = [0]

    def give(px, pz, **to):
        i = sends[0]
        sends[0] += 1
        begin(xd.at[px, c, pz], xd.at[px, c, pz], g_s.at[i], g_r.at[px, c, pz], **to)

    def arrive(px, pc, pz):
        landed(xd.at[px, pc, pz], g_r.at[px, pc, pz])

    for k in FAR_FIRST:
        give(x, z, dz=k)
    give(x, z, dx=1)
    give(x, z, dx=-1)
    give(x, z, flip=1)
    mix = jax.nn.sigmoid(jnp.sum(ffn_in.astype(F32) * mix_w[...], axis=-1, keepdims=True))
    mix_row = jnp.sum(jnp.where(eye, jnp.broadcast_to(mix, (SEQ, SEQ)), 0.0), axis=0, keepdims=True)
    mix_mine = jnp.sum(jnp.where(mine, jnp.broadcast_to(mix_row, (SEQ, SEQ)), 0.0), axis=1, keepdims=True)

    def regroup(ref):
        return dot(perm[...], ref[...].reshape(128, Q)).astype(BF16).reshape(8, SEQ, Q)

    for i, (dx, flip) in enumerate(plane):
        landed(m1r.at[other(-dx, flip)], m1_q.at[i])
    m2s[...] = regroup(m1r)
    for k in FAR_FIRST:
        begin(m2s.at[up(z, k, NZ)], my.at[t, z], m2_s.at[k - 1], m2_q.at[k - 1], dz=k)
    my[t, z] = m2s[z]

    for k in Z_ORDER[1:]:
        pz = up(z, k, NZ)
        arrive(x, c, pz)
        give(x, pz, dx=1)
        give(x, pz, dx=-1)
        give(x, pz, flip=1)

    loaded("dg", "du", "eg", "eu", *[f"dd{q}" for q in range(NY)])
    quarter = (lax.broadcasted_iota(jnp.int32, (256, 1), 0) >> 2) & 3
    low_rows = (lax.broadcasted_iota(jnp.int32, (128, 1), 0) & 7) < 4

    def by_quarter(value):
        return jnp.concatenate(
            [jnp.where(quarter == q, value, jnp.zeros_like(value)) for q in range(NY)], axis=1
        )

    def dense_rows(k):
        px = up(x, k, NX)
        for pz in range(NZ):
            arrive(px, 1 - c, pz)
        both = dot(by_quarter(xd[px].reshape(256, Q)), wd[...]).reshape(16, 2, 8, 2 * FF)
        half = (both[:, 0] + both[:, 1]).reshape(128, 2 * FF)
        full = half + jnp.where(low_rows, pltpu.roll(half, 124, 0), pltpu.roll(half, 4, 0))
        hidden = (jax.nn.silu(full[:, 0:FF]) * full[:, FF:]).reshape(16, 8, FF)
        rows16 = jnp.concatenate([hidden, hidden], axis=1).astype(BF16).reshape(256, FF)
        part = dot(by_quarter(rows16), ddq[...].reshape(NY * FF, Q))
        s0[k] = jnp.where(c == 0, part[128:], part[0:128]).astype(BF16)
        begin(s0.at[k], r0.at[k], s0_s.at[k], s0_r.at[k], flip=1)
        own[k] = jnp.where(c == 0, part[0:128], part[128:])

    count = [0]

    def pass_on(pt, pz, dy):
        i = count[0]
        count[0] += 1
        begin(my.at[pt, pz], my.at[pt, pz], my_s.at[i], my_r.at[pt, pz], dy=dy)

    for k in Z_ORDER:
        pz = up(z, k, NZ)
        if k:
            landed(my.at[t, pz], m2_q.at[(-k) % NZ - 1])
        pass_on(t, pz, 1)
        pass_on(t, pz, -1)

    for m, k in enumerate(Z_ORDER):
        pz = up(z, k, NZ)
        for way in (1, -1):
            px = up(x, -way, NX)
            arrive(px, c, pz)
            if (m % 2 == 0) == (way == 1):
                give(px, pz, dx=way)
            give(px, pz, flip=1)
    dense_rows(0)
    for m, k in enumerate(Z_ORDER):
        pz = up(z, k, NZ)
        for way in (1, -1):
            pt = up(t, -way, NY)
            landed(my.at[pt, pz], my_r.at[pt, pz])
            if (m % 2 == 0) == (way == 1):
                pass_on(pt, pz, way)
    dense_rows(1)
    for k in Z_ORDER:
        pz = up(z, k, NZ)
        px = up(x, 2, NX)
        arrive(px, c, pz)
        give(px, pz, flip=1)
    dense_rows(3)

    left = slice(0, Q // 2)
    right = slice(Q // 2, Q)

    def x_send(i, value, dx):
        s1[i] = value.astype(BF16)
        begin(s1.at[i], r1.at[i], s1_s.at[i], s1_r.at[i], dx=dx)

    def x_got(i):
        landed(r1.at[i], s1_r.at[i])
        return r1[i].astype(F32)

    def joined(k):
        landed(r0.at[k], s0_r.at[k])
        own[k] = own[k] + r0[k].astype(F32)

    joined(1)
    x_send(2, own[1, :, right], 1)
    dense_rows(2)
    joined(3)
    x_send(3, own[3, :, left], -1)
    joined(0)


    for k in Z_ORDER:
        pz = up(z, k, NZ)
        pt = up(t, 2, NY)
        landed(my.at[pt, pz], my_r.at[pt, pz])
    rows_in = jnp.concatenate([my[k].reshape(128, Q) for k in range(NY)], axis=1).astype(F32)
    both = dot(rms_rows(rows_in, gain[...]).astype(BF16), we[...])
    hx[t] = (jax.nn.silu(both[:, 0:FF]) * both[:, FF:]).astype(BF16)
    for k in (2, 1, 3):
        begin(hx.at[t], hx.at[t], x_s.at[k - 1], x_r.at[k - 1], dy=k)

    joined(2)
    x_send(0, own[2, :, left], 1)
    x_send(1, own[2, :, right], -1)
    x_send(4, own[1, :, left] + x_got(0), 1)
    x_send(5, own[3, :, right] + x_got(1), -1)

    own_q = pl.ds(pl.multiple_of(t * Q, Q), Q)
    edx[t] = ed[:, own_q]
    for k in (1, 3, 2):
        src = up(t, -k, NY)
        landed(edx.at[src], ed_r.at[k - 1])
        landed(hx.at[src], x_r.at[k - 1])
    result = jnp.zeros((128, Q), F32)
    for k in range(NY):
        result = result + dot(hx[k], edx[k]).astype(BF16).astype(F32)
    eo[...] = result.astype(BF16).reshape(NZ, SEQ, Q)
    for k in FAR_FIRST:
        begin(eo.at[up(z, k, NZ)], n1r.at[z], n1_s.at[k - 1], n1_q.at[k - 1], dz=k)
    n1r[z] = eo[z]

    from_sides = [own[0, :, left] + x_got(3), own[0, :, right] + x_got(2)]
    sums = jnp.concatenate([from_sides[0] + x_got(4), from_sides[1] + x_got(5)], axis=1)
    bsum[...] = sums.reshape(NZ, SEQ, Q)
    s2[...] = sums.astype(BF16).reshape(NZ, SEQ, Q)
    for k in FAR_FIRST:
        begin(s2.at[up(z, k, NZ)], r2.at[k - 1], s2_s.at[k - 1], s2_r.at[k - 1], dz=k)

    for k in reversed(FAR_FIRST):
        landed(n1r.at[up(z, -k, NZ)], n1_q.at[k - 1])
    n2s[...] = regroup(n1r)
    for i, (dx, flip) in enumerate(plane):
        begin(n2s.at[other(dx, flip)], n2r.at[xc], n2_s.at[i], n2_q.at[i], dx=dx, flip=flip)
    n2r[xc] = n2s[xc]

    for k in reversed(FAR_FIRST):
        landed(r2.at[k - 1], s2_r.at[k - 1])
    dense = bsum[z]
    for k in range(NZ - 1):
        dense = dense + r2[k].astype(F32)
    dense = dense * mix_mine
    for q in range(NY):
        four = dense[4 * q : 4 * q + 4, :]
        ys[q] = jnp.concatenate([four, four], axis=0)
    yr[t] = ys[t]
    for k in (2, 1, 3):
        begin(ys.at[up(t, k, NY)], yr.at[t], y_s.at[k - 1], y_r.at[k - 1], dy=k)

    for i, (dx, flip) in enumerate(plane):
        landed(n2r.at[other(-dx, flip)], n2_q.at[i])
    back = n2r[...].reshape(128, Q)
    final = stream_cols.astype(F32)
    moe = w_cols[0] * dot(chosen[0], back) + w_cols[1] * dot(chosen[1], back)
    for k in (1, 3, 2):
        src = up(t, -k, NY)
        landed(yr.at[src], y_r.at[k - 1])
    dense_cols = jnp.concatenate([yr[k, 0:4, :] for k in range(NY)], axis=0)
    out[...] = final + moe + dense_cols

    for copy in done + started:
        copy.wait_send()


def layer(*operands):
    vmem = pl.BlockSpec(memory_space=pltpu.VMEM)
    hbm = pl.BlockSpec(memory_space=pltpu.HBM)
    dma = lambda *n: pltpu.SemaphoreType.DMA(n)
    buf = lambda shape, kind=BF16: pltpu.VMEM(shape, kind)
    return pl.pallas_call(
        layer_kernel,
        out_shape=(
            pltpu.VMEM((SEQ, Q), F32),
            pltpu.VMEM((SEQ, 2 * HEAD_DIM), BF16),
        ),
        in_specs=[hbm] * len(operands),
        out_specs=(vmem, vmem),
        scratch_shapes=[
            buf((SEQ, D)),
            buf((1, SEQ), jnp.int32),
            buf((SEQ, 512, 2 * HEAD_DIM)),
            buf((1, D), F32),
            buf((D, Q + 2 * HEAD_DIM)),
            buf((1, 4), F32),
            buf((1, HEAD_DIM), F32),
            buf((1, D), F32),
            buf((2, SEQ), jnp.int32),
            buf((2, SEQ), F32),
            buf((1, D), F32),
            buf((1, HEAD_DIM), F32),
            buf((SEQ, 8, HEAD_DIM), F32),
            buf((SEQ, HEAD_DIM), F32),
            buf((SEQ, HEAD_DIM), F32),
            buf((SEQ, HEAD_DIM), F32),
            buf((SEQ, 8, HEAD_DIM), F32),
            buf((SEQ, Q)),
            buf((D, Q)),
            buf((D, 2 * FF)),
            buf((D, 2 * FF)),
            buf((NY, FF, Q)),
            buf((FF, D)),
            buf((NY, FF, Q)),
            buf((NY, SEQ, Q)),
            buf((NY, SEQ, Q)),
            buf((128, 128)),
            buf((8, SEQ, Q)),
            buf((8, SEQ, Q)),
            buf((8, SEQ, Q)),
            buf((NY, NZ, SEQ, Q)),
            buf((NY, 128, FF)),
            buf((8, SEQ, Q)),
            buf((8, SEQ, Q)),
            buf((8, SEQ, Q)),
            buf((8, SEQ, Q)),
            buf((NX, NC, NZ, SEQ, Q)),
            buf((NX, NZ * SEQ, Q)),
            buf((NX, NZ * SEQ, Q)),
            buf((NX, NZ * SEQ, Q), F32),
            buf((6, NZ * SEQ, Q // 2)),
            buf((6, NZ * SEQ, Q // 2)),
            buf((NZ, SEQ, Q), F32),
            buf((NZ, SEQ, Q)),
            buf((NZ - 1, SEQ, Q)),
            buf((NY, 8, Q), F32),
            buf((NY, 8, Q), F32),
            dma(27),
            dma(3), dma(3), dma(3), dma(3), dma(3), dma(3), dma(3), dma(3), dma(3), dma(3),
            dma(N_SENDS), dma(NX, NC, NZ),
            dma(7), dma(7), dma(7), dma(7),
            dma(24), dma(NY, NZ),
            dma(7), dma(7), dma(7), dma(7),
            dma(4), dma(4), dma(6), dma(6), dma(7), dma(7),
        ],
        compiler_params=pltpu.CompilerParams(
            collective_id=0, has_side_effects=True, vmem_limit_bytes=60 * 1024 * 1024
        ),
        name="layer",
    )(*operands)


def on_device(
    residual_in, lengths, kv_cache, norm_gain_attn, query_weight, key_weight, value_weight,
    diff_lambda, head_gain, out_weight, norm_gain_ffn, route_ids, route_weights, expert_gate,
    expert_up, expert_down, dense_gate, dense_up, dense_down, dense_mix,
):
    width = residual_in.shape[1]
    half = QK_DIM // 2
    inverse = 10000.0 ** (-np.arange(half, dtype=np.float32) / np.float32(half))
    inverse = np.tile(inverse.astype(np.float32), 4)[None, :]
    final, fresh = layer(
        residual_in,
        lengths.reshape(1, -1),
        kv_cache.reshape(SEQ, 512, 2 * HEAD_DIM),
        norm_gain_attn.reshape(1, width),
        query_weight,
        key_weight,
        value_weight,
        diff_lambda.reshape(1, -1),
        head_gain.reshape(1, -1),
        out_weight,
        norm_gain_ffn.reshape(1, width),
        route_ids.T,
        route_weights.T,
        expert_gate.reshape(width, -1),
        expert_up.reshape(width, -1),
        expert_down.reshape(-1, width),
        dense_gate,
        dense_up,
        dense_down,
        dense_mix.reshape(1, width),
        jnp.asarray(inverse),
    )
    return (final.astype(BF16), fresh.reshape(SEQ, 1, 2 * HEAD_DIM))


def solution(mesh):
    placed = (
        P("ep", None),
        P("ep"),
        P("ep", "tp", None, None),
        P(),
        P(None, "tp"),
        P(None, "tp"),
        P(None, "tp"),
        P("tp"),
        P(),
        P(None, "tp"),
        P(),
        P("ep", None),
        P("ep", None),
        P("ep", None, "tp"),
        P("ep", None, "tp"),
        P("ep", "tp", None),
        P(None, "ep"),
        P(None, "ep"),
        P("ep", None),
        P(),
    )
    return jax.shard_map(
        on_device,
        mesh=mesh,
        in_specs=placed,
        out_specs=(P("ep", "tp"), P("ep", "tp", None)),
        check_vma=False,
    )
```

```python
import jax
import jax.numpy as jnp
import numpy as np
from jax import lax
from jax.experimental import pallas as pl
from jax.experimental.pallas import tpu as pltpu
from jax.sharding import PartitionSpec as P

QK_DIM = 64
HEAD_DIM = 128
EPS = 1e-06
MESH = pl.DeviceIdType.MESH
F32 = jnp.float32
BF16 = jnp.bfloat16
NX, NZ, NY, NC = 4, 8, 4, 2
SEQ = 16
D = 2048
Q = 512
FF = 128
Z_ORDER = (0, -1, 1, -2, 2, -3, 3, 4)
FAR_FIRST = (4, 3, 5, 2, 6, 1, 7)
N_SENDS = 56


def rms_rows(values, gain):
    mean_sq = jnp.mean(values * values, axis=-1, keepdims=True)
    return values * lax.rsqrt(mean_sq + EPS) * gain


def dot(a, b):
    return jnp.dot(a, b, preferred_element_type=F32)


def up(v, n, size, dynamic=False):
    return lax.rem(v + (n if dynamic else n % size), size)


def layer_kernel(
    resid_h, lens_h, kv_h, ga_h, wq_h, wk_h, wv_h, lam_h, hgain_h, wo_h, gf_h, ids_h, rw_h,
    eg_h, eu_h, ed_h, dg_h, du_h, dd_h, mixw_h, inv_h, out, rows_out,
    resid, lens, kv, gain_a, wqkv, lam, hgain, gain, ids_t, rw_t, mix_w, inv,
    qs, fk, fv, lenb, mixed, heads,
    wo, we, wd, ddq, ed, edx, hg, sg, perm, m1s, m1r, m2s, my, hx, eo, n1r, n2s, n2r,
    xd, cut, join, piece, raw, s0, r0, own, s1, r1, bsum, s2, r2, ys, yr,
    lsem, ed_s, ed_r, h_s, h_r, c_s, c_r, x_s, x_r, y_s, y_r, g_s, g_r, p_s, p_r, m1_s, m1_q, m2_s, m2_q,
    my_s, my_r, n1_s, n1_q, n2_s, n2_q, s0_s, s0_r, s1_s, s1_r, s2_s, s2_r,
):
    e = lax.axis_index("ep")
    t = lax.axis_index("tp")
    z = lax.div(e, 8)
    x = lax.rem(lax.div(e, 2), 4)
    c = lax.rem(e, 2)

    def dev(dz=0, dx=0, flip=0, dy=0):
        cc = 1 - c if flip else c
        return {
            "ep": (up(z, dz, NZ) * NX + up(x, dx, NX)) * NC + cc,
            "tp": up(t, dy, NY),
        }

    def remote(src, dst, ssem, rsem, to):
        return pltpu.make_async_remote_copy(
            src_ref=src, dst_ref=dst, send_sem=ssem, recv_sem=rsem, device_id=to, device_id_type=MESH
        )

    pairs = {
        "lens": (lens_h, lens),
        "inv": (inv_h, inv),
        "ids": (ids_h, ids_t),
        "rw": (rw_h, rw_t),
        "resid": (resid_h, resid),
        "gain_a": (ga_h, gain_a),
        "wq": (wq_h, wqkv.at[:, pl.ds(0, Q)]),
        "wk": (wk_h, wqkv.at[:, pl.ds(Q, HEAD_DIM)]),
        "wv": (wv_h, wqkv.at[:, pl.ds(Q + HEAD_DIM, HEAD_DIM)]),
        "lam": (lam_h, lam),
        "hgain": (hgain_h, hgain),
    }
    for g in range(4):
        pairs[f"kv{g}"] = (kv_h.at[pl.ds(4 * g, 4)], kv.at[pl.ds(4 * g, 4)])
    pairs |= {
        "wo": (wo_h, wo),
        "gain": (gf_h, gain),
        "mix": (mixw_h, mix_w),
        "ed": (ed_h, ed),
        "dg": (dg_h, wd.at[:, pl.ds(0, FF)]),
        "du": (du_h, wd.at[:, pl.ds(FF, FF)]),
        "eg": (eg_h, we.at[:, pl.ds(0, FF)]),
        "eu": (eu_h, we.at[:, pl.ds(FF, FF)]),
    }
    for q in range(NY):
        pairs[f"dd{q}"] = (dd_h.at[:, pl.ds(q * Q, Q)], ddq.at[q])
    loads = {
        name: pltpu.make_async_copy(a, b, lsem.at[i]) for i, (name, (a, b)) in enumerate(pairs.items())
    }
    for load in loads.values():
        load.start()

    def loaded(*names):
        for name in names:
            loads[name].wait()

    barrier = pltpu.get_barrier_semaphore()
    peers = (
        [dev(dy=k) for k in (1, 2, 3)]
        + [dev(dx=k) for k in (1, 2, 3)]
        + [dev(dz=k) for k in range(1, 8)]
        + [dev(dx=k, flip=1) for k in (0, 1, 2, 3)]
        + [dev(dz=k, dy=j) for k in range(1, 8) for j in (1, 2, 3)]
    )
    for peer in peers:
        pl.semaphore_signal(barrier, inc=1, device_id=peer, device_id_type=MESH)

    loaded("lens", "inv", "ids", "rw")

    ids = ids_t[...]
    place = ((ids >> 1) & 3) * (NC * NZ * 2) + (ids & 1) * (NZ * 2) + (ids >> 3) * 2
    row16 = lax.broadcasted_iota(jnp.int32, (SEQ, SEQ), 0)
    col16 = lax.broadcasted_iota(jnp.int32, (SEQ, SEQ), 1)
    eye = row16 == col16

    def column(rows, k):
        spread = jnp.broadcast_to(rows[k : k + 1, :], (SEQ, SEQ))
        return jnp.sum(jnp.where(eye, spread, 0.0), axis=1, keepdims=True)

    lane_f = lax.broadcasted_iota(jnp.int32, (SEQ, 128), 1).astype(F32)
    rw = rw_t[...]
    w_cols = [column(rw, k) for k in (0, 1)]
    place_cols = [column(place.astype(F32), k) for k in (0, 1)]
    member = [jnp.where(lane_f == col, 1.0, 0.0) for col in place_cols]
    before = jnp.where(row16 > col16, 1.0, 0.0).astype(BF16)
    earlier = dot(before, (member[0] + member[1]).astype(BF16))
    chosen = []
    for k in (0, 1):
        slot = jnp.sum(member[k] * earlier, axis=1, keepdims=True)
        chosen.append(jnp.where(lane_f == place_cols[k] + slot, 1.0, 0.0).astype(BF16))
    prow = lax.broadcasted_iota(jnp.int32, (128, 128), 0)
    pcol = lax.broadcasted_iota(jnp.int32, (128, 128), 1)
    swapped = ((prow >> 1) & 7) * 16 + (prow >> 4) * 2 + (prow & 1)
    perm[...] = jnp.where(pcol == swapped, 1.0, 0.0).astype(BF16)
    orow = lax.broadcasted_iota(jnp.int32, (64, SEQ), 0)
    ocol = lax.broadcasted_iota(jnp.int32, (64, SEQ), 1)
    token_of = (orow >> 4) * 4 + (orow & 3) == ocol
    for j in range(4):
        cut[j] = jnp.where(token_of & (((orow >> 2) & 3) == j), 1.0, 0.0).astype(BF16)
    jrow = lax.broadcasted_iota(jnp.int32, (256, 256), 0)
    jcol = lax.broadcasted_iota(jnp.int32, (256, 256), 1)
    source = ((jrow >> 4) & 3) * 64 + ((jrow >> 2) & 3) * 16 + (jrow >> 6) * 4 + (jrow & 3)
    join[...] = jnp.where(jcol == source, 1.0, 0.0).astype(BF16)
    low8 = lax.broadcasted_iota(jnp.int32, (8, 128), 0) < 4

    lane1 = lax.broadcasted_iota(jnp.int32, (SEQ, HEAD_DIM), 1)
    length = column(lens[...].astype(F32), 0)
    lenb[...] = jnp.broadcast_to(length, (SEQ, HEAD_DIM))
    angle = length * inv[...]
    cosine = jnp.cos(angle)
    low = lax.rem(lane1, QK_DIM) < QK_DIM // 2
    sine = jnp.where(low, -jnp.sin(angle), jnp.sin(angle))

    def turned(v):
        ahead = pltpu.roll(v, HEAD_DIM - QK_DIM // 2, 1)
        behind = pltpu.roll(v, QK_DIM // 2, 1)
        return (v * cosine + jnp.where(low, ahead, behind) * sine).astype(BF16)

    loaded("resid", "gain_a")
    normed = rms_rows(resid[...].astype(F32), gain_a[...]).astype(BF16)
    loaded("wq", "wk", "wv", "lam", "hgain")
    proj = dot(normed, wqkv[...])
    key_new = turned(proj[:, Q : Q + HEAD_DIM])
    val_new = proj[:, Q + HEAD_DIM :].astype(BF16)
    rows_out[:, 0:HEAD_DIM] = key_new
    rows_out[:, HEAD_DIM:] = val_new
    fk[...] = key_new.astype(F32)
    fv[...] = val_new.astype(F32)
    first = lane1 < QK_DIM
    turned_q = [turned(proj[:, j * HEAD_DIM : (j + 1) * HEAD_DIM]) for j in range(4)]
    zero = jnp.zeros((SEQ, HEAD_DIM), BF16)
    stack = jnp.concatenate(
        [jnp.where(first, q, zero) for q in turned_q] + [jnp.where(first, zero, q) for q in turned_q],
        axis=0,
    )
    to_seq = lax.rem(prow, 8) * SEQ + lax.div(prow, 8) == pcol
    to_head = lax.rem(prow, SEQ) * 8 + lax.div(prow, SEQ) == pcol
    qs[...] = dot(jnp.where(to_seq, 1.0, 0.0).astype(BF16), stack).reshape(SEQ, 8, HEAD_DIM)

    srow = lax.broadcasted_iota(jnp.int32, (8, 4), 0)
    scol = lax.broadcasted_iota(jnp.int32, (8, 4), 1)
    lam_col = jnp.sum(
        jnp.where(srow - 4 == scol, jnp.broadcast_to(lam[...], (8, 4)), 0.0), axis=1, keepdims=True
    )
    sign = jnp.where(lax.broadcasted_iota(jnp.int32, (8, 1), 0) < 4, 1.0, -lam_col)
    sign4 = jnp.concatenate([sign] * 4, axis=0)
    position = lax.broadcasted_iota(jnp.int32, (32, 512), 1).astype(F32)
    scale = QK_DIM ** (-0.5)
    contract_last = (((1,), (1,)), ((), ()))
    loaded("kv0", "kv1", "kv2", "kv3")
    for g in range(4):
        seqs = range(4 * g, 4 * g + 4)
        q4 = [qs[b] for b in seqs]
        scores = jnp.concatenate(
            [
                lax.dot_general(
                    q.astype(BF16), kv[b, :, 0:HEAD_DIM], contract_last, preferred_element_type=F32
                )
                for q, b in zip(q4, seqs)
            ],
            axis=0,
        )
        latest = scale * jnp.concatenate(
            [jnp.sum(q * fk[b : b + 1, :], axis=1, keepdims=True) for q, b in zip(q4, seqs)], axis=0
        )
        count = jnp.concatenate([jnp.broadcast_to(lenb[b : b + 1, 0:1], (8, 1)) for b in seqs], axis=0)
        masked = jnp.where(position < count, scores * scale, -1e30)
        top = jnp.maximum(jnp.max(masked, axis=1, keepdims=True), latest)
        raised = jnp.exp(masked - top)
        raised_new = jnp.exp(latest - top)
        weight = sign4 / (jnp.sum(raised, axis=1, keepdims=True) + raised_new)
        both = raised * weight
        mapped = (both + pltpu.roll(both, 28, 0)).astype(BF16)
        new = jnp.broadcast_to(raised_new * weight, (32, HEAD_DIM))
        mapped_new = (new + pltpu.roll(new, 28, 0)).astype(BF16).astype(F32)
        for i, b in enumerate(seqs):
            at = slice(8 * i, 8 * i + 8)
            mixed[b] = dot(mapped[at, :], kv[b, :, HEAD_DIM:]) + mapped_new[at, :] * fv[b : b + 1, :]
    normed_heads = rms_rows(mixed[...].reshape(128, HEAD_DIM), hgain[...]).astype(BF16)
    by_head = dot(jnp.where(to_head, 1.0, 0.0).astype(BF16), normed_heads).astype(BF16)
    for j in range(4):
        heads[:, j * HEAD_DIM : (j + 1) * HEAD_DIM] = by_head[j * SEQ : (j + 1) * SEQ, :]

    pl.semaphore_wait(barrier, 38)

    heads_out = [
        remote(heads, hg.at[t], h_s.at[k - 1], h_r.at[k - 1], dev(dy=k)) for k in (1, 2, 3)
    ]
    for copy in heads_out:
        copy.start()
    own_cols = pl.ds(pl.multiple_of(t * Q, Q), Q)
    loaded("wo", "gain", "mix", "ed")

    def wo_rows(src):
        return wo[pl.ds(pl.multiple_of(src * Q, Q), Q), :]

    total = resid[:, own_cols].astype(F32) + dot(heads[...], wo_rows(t))
    for k in (1, 3, 2):
        src = up(t, -k, NY)
        remote(heads, hg.at[src], h_s.at[k - 1], h_r.at[k - 1], dev()).wait_recv()
        total = total + dot(hg[src], wo_rows(src))
    stream_cols = total.astype(BF16)
    sg[t] = stream_cols
    done = heads_out
    started = []

    def begin(src, dst, ssem, rsem, **to):
        copy = remote(src, dst, ssem, rsem, dev(**to))
        copy.start()
        started.append(copy)

    def landed(ref, rsem):
        remote(ref, ref, rsem, rsem, dev()).wait_recv()

    cols128 = [stream_cols[:, j * 128 : (j + 1) * 128] for j in range(4)]
    cutting = sum(dot(cut[j], cols128[j]) for j in range(4))
    piece[...] = cutting.astype(BF16).reshape(NY, SEQ, 128)
    sent = 0
    for dz in FAR_FIRST + (0,):
        for dy in (2, 1, 3, 0):
            if dz or dy:
                src = piece.at[up(t, dy, NY)]
                begin(src, raw.at[z, t], p_s.at[sent], p_r.at[z, t], dz=dz, dy=dy)
                sent += 1
    raw[z, t] = piece[t]

    xc = x * NC + c
    outgoing = lax.dot_general(
        (chosen[0] + chosen[1]), stream_cols, (((0,), (0,)), ((), ())), preferred_element_type=F32
    )
    m1s[...] = outgoing.astype(BF16).reshape(NX * NC, SEQ, Q)
    plane = [(dx, flip) for dx in (2, 1, 3) for flip in (0, 1)] + [(0, 1)]

    def other(dx, flip):
        return up(x, dx, NX) * NC + (1 - c if flip else c)

    for i, (dx, flip) in enumerate(plane):
        begin(m1s.at[other(dx, flip)], m1r.at[xc], m1_s.at[i], m1_q.at[i], dx=dx, flip=flip)
    m1r[xc] = m1s[xc]
    for k in (2, 1, 3):
        begin(sg.at[t], sg.at[t], c_s.at[k - 1], c_r.at[k - 1], dy=k)
    for k in (2, 1, 3):
        cols = pl.ds(pl.multiple_of(up(t, k, NY) * Q, Q), Q)
        begin(ed.at[:, cols], edx.at[t], ed_s.at[k - 1], ed_r.at[k - 1], dy=k)

    gains = [gain[:, i * 128 : (i + 1) * 128] for i in range(16)]
    gain8 = jnp.concatenate(
        [jnp.where(low8, gains[2 * i], gains[2 * i + 1]) for i in range(8)], axis=0
    ).reshape(1, 8, 8, 128)
    sends = [0]

    def give(px, pz, **to):
        i = sends[0]
        sends[0] += 1
        begin(xd.at[px, c, pz], xd.at[px, c, pz], g_s.at[i], g_r.at[px, c, pz], **to)

    def arrive(px, pc, pz):
        landed(xd.at[px, pc, pz], g_r.at[px, pc, pz])

    def regroup(ref):
        return dot(perm[...], ref[...].reshape(128, Q)).astype(BF16).reshape(8, SEQ, Q)

    for i, (dx, flip) in enumerate(plane):
        landed(m1r.at[other(-dx, flip)], m1_q.at[i])
    m2s[...] = regroup(m1r)
    for k in FAR_FIRST:
        begin(m2s.at[up(z, k, NZ)], my.at[t, z], m2_s.at[k - 1], m2_q.at[k - 1], dz=k)
    my[t, z] = m2s[z]

    low32 = (lax.broadcasted_iota(jnp.int32, (32, 1), 0) & 7) < 4
    for ks in (Z_ORDER[:4], Z_ORDER[4:]):
        for k in ks:
            for j in range(NY):
                pz, pt = up(z, k, NZ), up(t, j, NY)
                if k or j:
                    landed(raw.at[pz, pt], p_r.at[pz, pt])
        four = jnp.concatenate([raw[up(z, k, NZ)].reshape(64, 128) for k in ks], axis=0).astype(F32)
        four = four.reshape(4, 8, 8, 128)
        square = jnp.sum(four * four, axis=1).reshape(32, 128)
        square = square + jnp.where(low32, pltpu.roll(square, 28, 0), pltpu.roll(square, 4, 0))
        mean_sq = jnp.sum(square, axis=1, keepdims=True) * (1.0 / D)
        root = jnp.broadcast_to(lax.rsqrt(mean_sq + EPS), (32, 128)).reshape(4, 1, 8, 128)
        ready = (four * root * gain8).reshape(256, 128).astype(BF16)
        laid = dot(join[...], ready).astype(BF16)
        wide = jnp.concatenate([laid[j * 64 : (j + 1) * 64] for j in range(4)], axis=1)
        for i, k in enumerate(ks):
            pz = up(z, k, NZ)
            xd[x, c, pz] = wide[i * SEQ : (i + 1) * SEQ]
            give(x, pz, dx=1)
            give(x, pz, dx=-1)
            give(x, pz, flip=1)

    loaded("dg", "du", "eg", "eu", *[f"dd{q}" for q in range(NY)])
    low_rows = (lax.broadcasted_iota(jnp.int32, (128, 1), 0) & 7) < 4

    def swapped_rows(value):
        return jnp.where(low_rows, pltpu.roll(value, 124, 0), pltpu.roll(value, 4, 0))

    def dense_rows(k):
        px = up(x, k, NX)
        for pz in range(NZ):
            arrive(px, 1 - c, pz)
        rows = xd[px].reshape(256, Q)
        part = [dot(rows, wd[q * Q : (q + 1) * Q, :]).reshape(16, 2, 8, 2 * FF) for q in range(NY)]
        even = (part[0][:, 0] + part[2][:, 1]).reshape(128, 2 * FF)
        odd = (part[1][:, 0] + part[3][:, 1]).reshape(128, 2 * FF)
        kept = jnp.where(low_rows, even, odd)
        full = kept + swapped_rows(kept)
        hidden = (jax.nn.silu(full[:, 0:FF]) * full[:, FF:]).astype(BF16)
        got = [dot(hidden, ddq[q]) for q in range(NY)]
        top = jnp.where(low_rows, got[0], got[1]).reshape(16, 1, 8, Q)
        bottom = jnp.where(low_rows, got[2], got[3]).reshape(16, 1, 8, Q)
        added = jnp.concatenate([top, bottom], axis=1).reshape(256, Q)
        s0[k] = jnp.where(c == 0, added[128:], added[0:128]).astype(BF16)
        begin(s0.at[k], r0.at[k], s0_s.at[k], s0_r.at[k], flip=1)
        own[k] = jnp.where(c == 0, added[0:128], added[128:])

    count = [0]

    def pass_on(pt, pz, dy):
        i = count[0]
        count[0] += 1
        begin(my.at[pt, pz], my.at[pt, pz], my_s.at[i], my_r.at[pt, pz], dy=dy)

    for k in Z_ORDER:
        pz = up(z, k, NZ)
        if k:
            landed(my.at[t, pz], m2_q.at[(-k) % NZ - 1])
        pass_on(t, pz, 1)
        pass_on(t, pz, -1)

    for m, k in enumerate(Z_ORDER):
        pz = up(z, k, NZ)
        for way in (1, -1):
            px = up(x, -way, NX)
            arrive(px, c, pz)
            if (m % 2 == 0) == (way == 1):
                give(px, pz, dx=way)
            give(px, pz, flip=1)
    dense_rows(0)
    dense_rows(1)
    dense_rows(3)
    for m, k in enumerate(Z_ORDER):
        pz = up(z, k, NZ)
        for way in (1, -1):
            pt = up(t, -way, NY)
            landed(my.at[pt, pz], my_r.at[pt, pz])
            if (m % 2 == 0) == (way == 1):
                pass_on(pt, pz, way)
    for k in Z_ORDER:
        pz = up(z, k, NZ)
        px = up(x, 2, NX)
        arrive(px, c, pz)
        give(px, pz, flip=1)

    left = slice(0, Q // 2)
    right = slice(Q // 2, Q)

    def x_send(i, value, dx):
        s1[i] = value.astype(BF16)
        begin(s1.at[i], r1.at[i], s1_s.at[i], s1_r.at[i], dx=dx)

    def x_got(i):
        landed(r1.at[i], s1_r.at[i])
        return r1[i].astype(F32)

    def joined(k):
        landed(r0.at[k], s0_r.at[k])
        own[k] = own[k] + r0[k].astype(F32)

    joined(1)
    x_send(2, own[1, :, right], 1)
    dense_rows(2)
    joined(3)
    x_send(3, own[3, :, left], -1)
    joined(0)


    for k in Z_ORDER:
        pz = up(z, k, NZ)
        pt = up(t, 2, NY)
        landed(my.at[pt, pz], my_r.at[pt, pz])
    rows_in = jnp.concatenate([my[k].reshape(128, Q) for k in range(NY)], axis=1).astype(F32)
    both = dot(rms_rows(rows_in, gain[...]).astype(BF16), we[...])
    hx[t] = (jax.nn.silu(both[:, 0:FF]) * both[:, FF:]).astype(BF16)
    for k in (2, 1, 3):
        begin(hx.at[t], hx.at[t], x_s.at[k - 1], x_r.at[k - 1], dy=k)

    joined(2)
    x_send(0, own[2, :, left], 1)
    x_send(1, own[2, :, right], -1)
    x_send(4, own[1, :, left] + x_got(0), 1)
    x_send(5, own[3, :, right] + x_got(1), -1)

    own_q = pl.ds(pl.multiple_of(t * Q, Q), Q)
    edx[t] = ed[:, own_q]
    for k in (1, 3, 2):
        src = up(t, -k, NY)
        landed(edx.at[src], ed_r.at[k - 1])
        landed(hx.at[src], x_r.at[k - 1])
    result = jnp.zeros((128, Q), F32)
    for k in range(NY):
        result = result + dot(hx[k], edx[k]).astype(BF16).astype(F32)
    eo[...] = result.astype(BF16).reshape(NZ, SEQ, Q)
    for k in FAR_FIRST:
        begin(eo.at[up(z, k, NZ)], n1r.at[z], n1_s.at[k - 1], n1_q.at[k - 1], dz=k)
    n1r[z] = eo[z]

    from_sides = [own[0, :, left] + x_got(3), own[0, :, right] + x_got(2)]
    sums = jnp.concatenate([from_sides[0] + x_got(4), from_sides[1] + x_got(5)], axis=1)
    bsum[...] = sums.reshape(NZ, SEQ, Q)
    s2[...] = sums.astype(BF16).reshape(NZ, SEQ, Q)
    for k in FAR_FIRST:
        begin(s2.at[up(z, k, NZ)], r2.at[k - 1], s2_s.at[k - 1], s2_r.at[k - 1], dz=k)

    for k in (1, 3, 2):
        src = up(t, -k, NY)
        landed(sg.at[src], c_r.at[k - 1])
    stream = jnp.concatenate([sg[k] for k in range(NY)], axis=1).astype(F32)
    ffn_in = rms_rows(stream, gain[...]).astype(BF16)
    mine = 4 * t + (row16 & 3) == col16
    mix = jax.nn.sigmoid(jnp.sum(ffn_in.astype(F32) * mix_w[...], axis=-1, keepdims=True))
    mix_row = jnp.sum(jnp.where(eye, jnp.broadcast_to(mix, (SEQ, SEQ)), 0.0), axis=0, keepdims=True)
    mix_mine = jnp.sum(jnp.where(mine, jnp.broadcast_to(mix_row, (SEQ, SEQ)), 0.0), axis=1, keepdims=True)
    for k in reversed(FAR_FIRST):
        landed(n1r.at[up(z, -k, NZ)], n1_q.at[k - 1])
    n2s[...] = regroup(n1r)
    for i, (dx, flip) in enumerate(plane):
        begin(n2s.at[other(dx, flip)], n2r.at[xc], n2_s.at[i], n2_q.at[i], dx=dx, flip=flip)
    n2r[xc] = n2s[xc]

    for k in reversed(FAR_FIRST):
        landed(r2.at[k - 1], s2_r.at[k - 1])
    dense = bsum[z]
    for k in range(NZ - 1):
        dense = dense + r2[k].astype(F32)
    dense = dense * mix_mine
    for q in range(NY):
        four = dense[4 * q : 4 * q + 4, :]
        ys[q] = jnp.concatenate([four, four], axis=0)
    yr[t] = ys[t]
    for k in (2, 1, 3):
        begin(ys.at[up(t, k, NY)], yr.at[t], y_s.at[k - 1], y_r.at[k - 1], dy=k)

    for i, (dx, flip) in enumerate(plane):
        landed(n2r.at[other(-dx, flip)], n2_q.at[i])
    back = n2r[...].reshape(128, Q)
    final = stream_cols.astype(F32)
    moe = w_cols[0] * dot(chosen[0], back) + w_cols[1] * dot(chosen[1], back)
    for k in (1, 3, 2):
        src = up(t, -k, NY)
        landed(yr.at[src], y_r.at[k - 1])
    dense_cols = jnp.concatenate([yr[k, 0:4, :] for k in range(NY)], axis=0)
    out[...] = final + moe + dense_cols

    for copy in done + started:
        copy.wait_send()


def layer(*operands):
    vmem = pl.BlockSpec(memory_space=pltpu.VMEM)
    hbm = pl.BlockSpec(memory_space=pltpu.HBM)
    dma = lambda *n: pltpu.SemaphoreType.DMA(n)
    buf = lambda shape, kind=BF16: pltpu.VMEM(shape, kind)
    return pl.pallas_call(
        layer_kernel,
        out_shape=(
            pltpu.VMEM((SEQ, Q), F32),
            pltpu.VMEM((SEQ, 2 * HEAD_DIM), BF16),
        ),
        in_specs=[hbm] * len(operands),
        out_specs=(vmem, vmem),
        scratch_shapes=[
            buf((SEQ, D)),
            buf((1, SEQ), jnp.int32),
            buf((SEQ, 512, 2 * HEAD_DIM)),
            buf((1, D), F32),
            buf((D, Q + 2 * HEAD_DIM)),
            buf((1, 4), F32),
            buf((1, HEAD_DIM), F32),
            buf((1, D), F32),
            buf((2, SEQ), jnp.int32),
            buf((2, SEQ), F32),
            buf((1, D), F32),
            buf((1, HEAD_DIM), F32),
            buf((SEQ, 8, HEAD_DIM), F32),
            buf((SEQ, HEAD_DIM), F32),
            buf((SEQ, HEAD_DIM), F32),
            buf((SEQ, HEAD_DIM), F32),
            buf((SEQ, 8, HEAD_DIM), F32),
            buf((SEQ, Q)),
            buf((D, Q)),
            buf((D, 2 * FF)),
            buf((D, 2 * FF)),
            buf((NY, FF, Q)),
            buf((FF, D)),
            buf((NY, FF, Q)),
            buf((NY, SEQ, Q)),
            buf((NY, SEQ, Q)),
            buf((128, 128)),
            buf((8, SEQ, Q)),
            buf((8, SEQ, Q)),
            buf((8, SEQ, Q)),
            buf((NY, NZ, SEQ, Q)),
            buf((NY, 128, FF)),
            buf((8, SEQ, Q)),
            buf((8, SEQ, Q)),
            buf((8, SEQ, Q)),
            buf((8, SEQ, Q)),
            buf((NX, NC, NZ, SEQ, Q)),
            buf((4, 64, SEQ)),
            buf((256, 256)),
            buf((NY, SEQ, 128)),
            buf((NZ, NY, SEQ, 128)),
            buf((NX, NZ * SEQ, Q)),
            buf((NX, NZ * SEQ, Q)),
            buf((NX, NZ * SEQ, Q), F32),
            buf((6, NZ * SEQ, Q // 2)),
            buf((6, NZ * SEQ, Q // 2)),
            buf((NZ, SEQ, Q), F32),
            buf((NZ, SEQ, Q)),
            buf((NZ - 1, SEQ, Q)),
            buf((NY, 8, Q), F32),
            buf((NY, 8, Q), F32),
            dma(27),
            dma(3), dma(3), dma(3), dma(3), dma(3), dma(3), dma(3), dma(3), dma(3), dma(3),
            dma(N_SENDS), dma(NX, NC, NZ), dma(31), dma(NZ, NY),
            dma(7), dma(7), dma(7), dma(7),
            dma(24), dma(NY, NZ),
            dma(7), dma(7), dma(7), dma(7),
            dma(4), dma(4), dma(6), dma(6), dma(7), dma(7),
        ],
        compiler_params=pltpu.CompilerParams(
            collective_id=0, has_side_effects=True, vmem_limit_bytes=60 * 1024 * 1024
        ),
        name="layer",
    )(*operands)


def on_device(
    residual_in, lengths, kv_cache, norm_gain_attn, query_weight, key_weight, value_weight,
    diff_lambda, head_gain, out_weight, norm_gain_ffn, route_ids, route_weights, expert_gate,
    expert_up, expert_down, dense_gate, dense_up, dense_down, dense_mix,
):
    width = residual_in.shape[1]
    half = QK_DIM // 2
    inverse = 10000.0 ** (-np.arange(half, dtype=np.float32) / np.float32(half))
    inverse = np.tile(inverse.astype(np.float32), 4)[None, :]
    final, fresh = layer(
        residual_in,
        lengths.reshape(1, -1),
        kv_cache.reshape(SEQ, 512, 2 * HEAD_DIM),
        norm_gain_attn.reshape(1, width),
        query_weight,
        key_weight,
        value_weight,
        diff_lambda.reshape(1, -1),
        head_gain.reshape(1, -1),
        out_weight,
        norm_gain_ffn.reshape(1, width),
        route_ids.T,
        route_weights.T,
        expert_gate.reshape(width, -1),
        expert_up.reshape(width, -1),
        expert_down.reshape(-1, width),
        dense_gate,
        dense_up,
        dense_down,
        dense_mix.reshape(1, width),
        jnp.asarray(inverse),
    )
    return (final.astype(BF16), fresh.reshape(SEQ, 1, 2 * HEAD_DIM))


def solution(mesh):
    placed = (
        P("ep", None),
        P("ep"),
        P("ep", "tp", None, None),
        P(),
        P(None, "tp"),
        P(None, "tp"),
        P(None, "tp"),
        P("tp"),
        P(),
        P(None, "tp"),
        P(),
        P("ep", None),
        P("ep", None),
        P("ep", None, "tp"),
        P("ep", None, "tp"),
        P("ep", "tp", None),
        P(None, "ep"),
        P(None, "ep"),
        P("ep", None),
        P(),
    )
    return jax.shard_map(
        on_device,
        mesh=mesh,
        in_specs=placed,
        out_specs=(P("ep", "tp"), P("ep", "tp", None)),
        check_vma=False,
    )
```
